256 devices in a mesh: ep: 16 (over y, x), tp: 16 (over z, core).
Axes of the slice: x: 4, y: 4, z: 8, core: 2. Of those that a mesh axis runs over, the one named last changes fastest.
Arguments:
- tokens: bfloat16 [16384, 2048], P('ep', 'tp'), may hold values from -48 to 48
- pre_gain: bfloat16 [2048], P('tp'), may hold values from 0.099609375 to 1.8984375
- route_ids: int32 [16384, 2], P('ep'), may hold values from 0 to 15, all different within a row; in each aligned block of 1024 rows (0 to 1023, 1024 to 2047, ...) at most 144 rows name the same one
- route_weights: float32 [16384, 2], P('ep'), may hold values from 0.1 to 1
- gate_weight: bfloat16 [16, 2048, 7168], P('ep', None, 'tp'), may hold values from -0.125 to 0.125
- up_weight: bfloat16 [16, 2048, 7168], P('ep', None, 'tp'), may hold values from -0.125 to 0.125
- down_weight: bfloat16 [16, 7168, 2048], P('ep', 'tp')
- post_gain: bfloat16 [2048], P('tp'), may hold values from 0.099609375 to 1.8984375
Outputs:
- mixed: bfloat16 [16384, 2048], P('ep', 'tp')
The draws below stay inside these ranges and needn't reach their ends.
Inputs may be any that keep to these rules, and one draw needn't show every extreme that they name: `route_ids`: each row names 2 different experts; among the rows of one index of ep no expert is named more than 144 times, a bound that some block reaches.
All inputs are finite; a program needn't handle non-finite values.
Results may differ from the reference program's by a relative error of at most 0.02.
Values may be sent and summed in bfloat16 or wider, within the bound.
A program may use at most 128 MiB of HBM per device.

```python
import math
import jax
import jax.numpy as jnp
import numpy as np
from jax import lax

D = 2048
FF = 7168
TOP = 2
TOK_DEV = 1024
EXPERTS = 16
TOKENS = 16384
CAP = 144
N_EP = 16
N_TP = 16


def column_profile(key):
    position = jnp.arange(D, dtype=jnp.float32) / D
    return 0.5 * jnp.exp(math.log(4.0) * position) * jax.random.uniform(key, (D,), jnp.float32, 0.6, 1.4)


def draw_tokens(key, part):
    first, second, third = jax.random.split(jax.random.fold_in(key, 11), 3)
    columns = column_profile(second)
    base = jnp.clip(jax.random.normal(first, (TOKENS, D), jnp.float32), -5.0, 5.0)
    row_scale = jnp.exp(jax.random.uniform(third, (TOKENS, 1), jnp.float32, math.log(0.3), math.log(3.0)))
    return (base * row_scale * columns[None, :]).astype(jnp.bfloat16)


def draw_down_weight(key, part):
    first, second = jax.random.split(jax.random.fold_in(key, 23), 2)
    columns = column_profile(second)
    base = jnp.clip(jax.random.normal(first, (EXPERTS, FF, D), jnp.float32), -5.0, 5.0)
    return (base * FF ** (-0.5) * columns[None, None, :]).astype(jnp.bfloat16)


def block_scale(rng, shape, cuts, least, top_value):
    def one(axis_at, parts):
        heights = jax.random.uniform(jax.random.fold_in(jax.random.fold_in(rng, 6), axis_at), (parts,), jnp.float32, least / len(cuts), top_value / len(cuts))
        return jnp.repeat(jnp.exp(heights), shape[axis_at] // parts).reshape((-1,) + (1,) * (len(shape) - axis_at - 1))

    factor_of = one(*cuts[0])
    for cut in cuts[1:]:
        factor_of = factor_of * one(*cut)
    return factor_of


def routed_block(key, own, number, rows, amount, top, most, skew):
    sequence = jax.random.permutation(key, amount)
    crowded, ordinary = portions_of(amount, rows * top, most, skew, True), portions_of(amount, rows * top, most, skew, False)
    places = jnp.arange(amount)

    def named(lengths, rotation):
        used = int((lengths > 0).sum())
        fixed = max(1, used // 4)
        passed = fixed + (places - fixed + rotation * (used - fixed)) % max(1, amount - fixed)
        return jnp.zeros((amount,), jnp.int32).at[sequence[jnp.where(places < fixed, places, passed)]].set(jnp.asarray(lengths, jnp.int32))

    lengths = jnp.where(number % 4 == 0, named(crowded, number // 4), named(ordinary, number - number // 4 - 1))
    mixed = jax.random.permutation(jax.random.fold_in(own, 3), amount)
    donor, receiver = mixed[0:amount // 2 * 2:2], mixed[1:amount // 2 * 2:2]
    room = jnp.minimum(lengths[donor] - 1, most - lengths[receiver]) // 2
    room = jnp.where((donor == sequence[0]) | (receiver == sequence[0]) | (lengths[receiver] == 0), 0, jnp.maximum(room, 0))
    passed = jax.random.randint(jax.random.fold_in(own, 4), (amount // 2,), 0, 1 << 20) % (room + 1)
    lengths = lengths.at[donor].add(-passed).at[receiver].add(passed)
    labels = jnp.searchsorted(jnp.cumsum(lengths), jnp.arange(rows * top), side="right").astype(jnp.int32)
    table = labels.reshape(top, rows).T
    table = table[jax.random.permutation(jax.random.fold_in(own, 1), rows)]
    rotation = jax.random.randint(jax.random.fold_in(own, 2), (rows, 1), 0, top)
    return jnp.take_along_axis(table, (jnp.arange(top)[None, :] + rotation) % top, axis=1)


def portions_of(amount, total, most, skew, full):
    loads = [(1 << 20) // math.isqrt(rank ** skew) + 1 for rank in range(1, amount + 1)]
    largest = most if full else min(most, max(-(-total // amount), total * loads[0] // sum(loads)))
    least = 1 if total - largest >= amount - 1 else 0
    counts, spare = [largest] + [least] * (amount - 1), total - largest - least * (amount - 1)
    while spare > 0:
        free = [i for i in range(1, amount) if counts[i] < largest] or [i for i in range(1, amount) if counts[i] < most]
        pool, budget = sum([loads[i] for i in free]), spare
        for i in free:
            addition = min(most - counts[i], max(1, budget * loads[i] // pool), spare)
            counts[i] = counts[i] + addition
            spare = spare - addition
    return np.array(counts)


def noise(stream_key, shape, deviation, most, pieces=(), kind=jnp.bfloat16):
    array = deviation * jax.random.normal(stream_key, shape, jnp.float32)
    if pieces:
        array = array * block_scale(stream_key, shape, pieces, -0.22, 0.18)
    return jnp.clip(array, -most, most).astype(kind)


def setup_inputs(seed: int = 0) -> dict:
    keys = jax.random.split(jax.random.key(seed), 9)
    tokens = draw_tokens(jax.random.fold_in(keys[8], 71), 0)
    pre_gain = jnp.clip(1.0 + 0.18 * jax.random.normal(keys[1], (D,), jnp.float32), 0.099609375, 1.8984375).astype(jnp.bfloat16)
    route_ids_keys = jax.random.split(jax.random.fold_in(keys[2], 1), TOKENS // TOK_DEV)
    route_ids_turns = jax.random.permutation(jax.random.fold_in(keys[2], 3), TOKENS // TOK_DEV)
    route_ids = jax.vmap(lambda own, number: routed_block(jax.random.fold_in(keys[2], 2), own, number, TOK_DEV, EXPERTS, TOP, CAP, 2))(route_ids_keys, route_ids_turns).reshape((TOKENS, TOP))
    route_weights = jnp.clip(jnp.exp(math.log(1.0) - 2.3025851 * jax.random.uniform(keys[3], (TOKENS, TOP), jnp.float32) ** block_scale(keys[3], (TOKENS, TOP), ((0, 16),), -0.2, 0.2)), 0.1, 1.0)
    gate_weight = noise(keys[4], (EXPERTS, D, FF), D ** -0.5, 0.125, ((0, 16), (2, 16)))
    up_weight = noise(keys[5], (EXPERTS, D, FF), D ** -0.5, 0.125, ((0, 16), (2, 16)))
    down_weight = draw_down_weight(jax.random.fold_in(keys[8], 71), 0)
    post_gain = jnp.clip(1.0 + 0.18 * jax.random.normal(keys[7], (D,), jnp.float32), 0.099609375, 1.8984375).astype(jnp.bfloat16)
    return dict(tokens=tokens, pre_gain=pre_gain, route_ids=route_ids, route_weights=route_weights, gate_weight=gate_weight, up_weight=up_weight, down_weight=down_weight, post_gain=post_gain)


epsilon = 1e-06

def reference(tokens, pre_gain, route_ids, route_weights, gate_weight, up_weight, down_weight, post_gain):
    values = tokens.astype(jnp.float32)
    normed = (values * lax.rsqrt(lax.optimization_barrier(jnp.mean(values * values, axis=1, keepdims=True)) + epsilon) * pre_gain.astype(jnp.float32)).astype(jnp.bfloat16)
    tok_total = tokens.shape[0]
    rows_total = N_EP * CAP
    hidden_units = FF // N_TP
    flat_ids = route_ids.reshape(-1).astype(jnp.int32)
    onehot = (flat_ids[:, None] == jnp.arange(EXPERTS, dtype=jnp.int32)[None, :]).astype(jnp.int32)
    slot_rank = lax.optimization_barrier(jnp.sum((jnp.cumsum(onehot, axis=0) - 1) * onehot, axis=1)).astype(jnp.int32)
    padded = jnp.concatenate([normed, jnp.zeros((1, D), jnp.bfloat16)], axis=0)
    positions = jnp.arange(tok_total * TOP, dtype=jnp.int32)

    def one_expert(expert):
        target = jnp.where(flat_ids == expert, slot_rank, rows_total).astype(jnp.int32)
        slot_table = jnp.full((rows_total,), tok_total * TOP, jnp.int32).at[target].set(positions, mode='drop')
        routed = padded[slot_table // TOP]
        gate_act = jnp.dot(routed, gate_weight[expert], preferred_element_type=jnp.float32)
        up_act = jnp.dot(routed, up_weight[expert], preferred_element_type=jnp.float32)
        hidden = (jax.nn.silu(gate_act) * up_act).astype(jnp.bfloat16)
        partials = jnp.einsum('rjf,jfd->jrd', hidden.reshape(rows_total, N_TP, hidden_units).astype(jnp.float32), down_weight[expert].reshape(N_TP, hidden_units, D).astype(jnp.float32))
        partials = lax.optimization_barrier(partials.astype(jnp.bfloat16)).astype(jnp.float32)
        return lax.optimization_barrier(jnp.sum(partials, axis=0)).astype(jnp.bfloat16)
    results = lax.map(one_expert, jnp.arange(EXPERTS, dtype=jnp.int32))
    copies = results.reshape(EXPERTS * rows_total, D)[flat_ids * rows_total + slot_rank]
    copies = copies.astype(jnp.float32).reshape(tok_total, TOP, D)
    combined = lax.optimization_barrier(jnp.sum(copies * route_weights[:, :, None], axis=1))
    scaled = combined * lax.rsqrt(lax.optimization_barrier(jnp.mean(combined * combined, axis=1, keepdims=True)) + epsilon)
    return (scaled * post_gain.astype(jnp.float32)).astype(jnp.bfloat16)
```

```python
import functools

import jax
import jax.numpy as jnp
from jax import lax
from jax.experimental import pallas as pl
from jax.experimental.pallas import tpu as pltpu
from jax.sharding import PartitionSpec as P

BF, F32 = jnp.bfloat16, jnp.float32
MESH = pl.DeviceIdType.MESH
NX = 4
EPS = 1e-06
LANES = 128
NT = (((1,), (1,)), ((), ()))


def near_first(i, n):
    return i if n < 4 else i + lax.div(i, 2) - 2 * lax.div(i, 3)


def kernel(
    dims,
    tokens, ids, weights, pre_gain, post_gain, gate_hbm, up_hbm, down_hbm,
    out,
    gates, downs, ranks, cols, outgoing, gains, x_all, x_norm, hidden,
    part, peer_part, ring_out, ring_in, results, returned, sums, squares, square_own,
    w_sem, gain_s, gain_r, disp_s, disp_r, ag_s, ag_r, d2d_s, d2d_r,
    pp_s, pp_r, rs_s, rs_r, ret_s, ret_r, sq_s, sq_r,
):
    ny, nx, nz, cap, per_chunk, width = dims
    n_ep, n_tp = ny * nx, nz * 2
    chunks = n_ep // per_chunk
    rows = cap * per_chunk
    half = rows // 2
    hops = nz // 2
    toks = tokens.shape[0]
    hid = gate_hbm.shape[0]
    hid_pad = downs.shape[0]

    ep, tp = lax.axis_index("ep"), lax.axis_index("tp")
    y, x = lax.div(ep, nx), lax.rem(ep, nx)
    z, core = lax.div(tp, 2), lax.rem(tp, 2)
    peer = z * 2 + 1 - core
    right = lax.rem(z + 1, nz) * 2 + core
    left = lax.rem(z + nz - 1, nz) * 2 + core

    def remote(src, dst, ssem, rsem, ep_to, tp_to):
        return pltpu.make_async_remote_copy(
            src_ref=src, dst_ref=dst, send_sem=ssem, recv_sem=rsem,
            device_id=(ep_to, tp_to), device_id_type=MESH,
        )

    barrier = pltpu.get_barrier_semaphore()

    def greet_ep(i, _):
        pl.semaphore_signal(barrier, inc=1, device_id=(lax.rem(ep + i, n_ep), tp), device_id_type=MESH)
        return 0

    def greet_tp(i, _):
        pl.semaphore_signal(barrier, inc=1, device_id=(ep, lax.rem(tp + i, n_tp)), device_id_type=MESH)
        return 0

    lax.fori_loop(1, n_ep, greet_ep, 0)
    lax.fori_loop(1, n_tp, greet_tp, 0)

    loads = (
        pltpu.make_async_copy(gate_hbm, gates.at[pl.ds(0, hid)], w_sem.at[0]),
        pltpu.make_async_copy(up_hbm, gates.at[pl.ds(hid_pad, hid)], w_sem.at[1]),
        pltpu.make_async_copy(down_hbm, downs.at[pl.ds(0, hid)], w_sem.at[2]),
    )
    for load in loads:
        load.start()
    if hid_pad > hid:
        gates[pl.ds(hid, hid_pad - hid), :] = jnp.zeros((hid_pad - hid, width), BF)
        gates[pl.ds(hid_pad + hid, hid_pad - hid), :] = jnp.zeros((hid_pad - hid, width), BF)
        downs[pl.ds(hid, hid_pad - hid), :] = jnp.zeros((hid_pad - hid, width), BF)
    gains[tp] = jnp.broadcast_to(pre_gain[...].astype(F32), (8, LANES))

    o_i = lax.broadcasted_iota(jnp.int32, (n_ep, toks), 0)
    a_i, b_i = o_i // nx, o_i % nx

    def near_vec(i, n):
        return i if n < 4 else jnp.where(i == 2, 3, jnp.where(i == 3, 2, i))

    e_of = ((y + near_vec(a_i, ny)) % ny) * nx + (x + near_vec(b_i, nx)) % nx
    first = (ids[0:1, :] == e_of).astype(F32)
    second = (ids[1:2, :] == e_of).astype(F32)
    named = first + second
    named_bf = named.astype(BF)
    step = min(256, toks)
    for at in range(0, toks, step):
        before = lax.broadcasted_iota(jnp.int32, (toks, step), 0)
        after = lax.broadcasted_iota(jnp.int32, (toks, step), 1) + at
        upper = jnp.where(before < after, 1.0, 0.0).astype(BF)
        ranks[:, pl.ds(at, step)] = jnp.dot(named_bf, upper, preferred_element_type=F32)
    rank = ranks[...]
    slot = o_i.astype(F32) * float(cap) + rank
    slot0 = jnp.sum(first * slot, axis=0, keepdims=True)
    slot1 = jnp.sum(second * slot, axis=0, keepdims=True)
    ranks[...] = jnp.where(named > 0.0, rank, -1.0)
    r8 = lax.broadcasted_iota(jnp.int32, (8, toks), 0)
    table = jnp.where(r8 == 0, slot0, jnp.where(r8 == 1, slot1, jnp.where(r8 == 2, weights[0:1, :], weights[1:2, :])))
    cols[...] = table.T

    pl.semaphore_wait(barrier, n_ep - 1 + n_tp - 1)

    def send_gain(i, _):
        remote(gains.at[tp], gains.at[tp], gain_s.at[i], gain_r.at[i], ep, lax.rem(tp + i, n_tp)).start()
        return 0

    lax.fori_loop(1, n_tp, send_gain, 0)

    def block_peer(o, sign):
        dy = near_first(lax.div(o, nx), ny)
        dx = near_first(lax.rem(o, nx), nx)
        return lax.rem(y + ny + sign * dy, ny) * nx + lax.rem(x + nx + sign * dx, nx)

    def block_rows(o):
        return pl.ds(pl.multiple_of(o * cap, 16), cap)

    def dispatch_copy(o):
        return remote(
            outgoing.at[o], x_all.at[tp, block_rows(o)], disp_s.at[o], disp_r.at[o], block_peer(o, 1), tp
        )

    s_i = lax.broadcasted_iota(jnp.int32, (cap, toks), 0).astype(F32)

    def dispatch(o, _):
        pick = jnp.where(s_i == ranks[pl.ds(o, 1), :], 1.0, 0.0).astype(BF)
        picked = jnp.dot(pick, tokens[...], preferred_element_type=F32).astype(BF)

        @pl.when(o == 0)
        def _():
            x_all[tp, pl.ds(0, cap)] = picked

        @pl.when(o > 0)
        def _():
            outgoing[o] = picked
            dispatch_copy(o).start()

        return 0

    lax.fori_loop(0, n_ep, dispatch, 0)

    def chunk_rows(c, at=0, count=None):
        return pl.ds(pl.multiple_of(c * rows + at, 16), rows if count is None else count)

    def slice_at(h):
        return lax.rem(z + 2 * nz - h, nz) * 2 + core

    def ag_copy(c, h, way):
        j = slice_at(h - 1 if way == 0 else 1 - h)
        at, count = (0, rows) if h < hops else ((0, half) if way == 0 else (half, half))
        ref = x_all.at[j, chunk_rows(c, at, count)]
        return remote(ref, ref, ag_s.at[c, way, h - 1], ag_r.at[c, way, h - 1], ep, right if way == 0 else left)

    def ag_arrived(c, h, way):
        j = slice_at(h if way == 0 else -h)
        at, count = (0, rows) if h < hops else ((0, half) if way == 0 else (half, half))
        ref = x_all.at[j, chunk_rows(c, at, count)]
        remote(ref, ref, ag_s.at[c, way, h - 1], ag_r.at[c, way, h - 1], ep, right).wait_recv()

    def d2d_copy(c, q):
        ref = x_all.at[slice_at(q), chunk_rows(c)]
        return remote(ref, ref, d2d_s.at[c, lax.rem(q + nz, nz)], d2d_r.at[c, lax.rem(q + nz, nz)], ep, peer)

    def d2d_arrived(c, q):
        j = lax.rem(z + 2 * nz - q, nz) * 2 + 1 - core
        ref = x_all.at[j, chunk_rows(c)]
        remote(ref, ref, d2d_s.at[c, q], d2d_r.at[c, q], ep, peer).wait_recv()

    def gather_first(c):
        for b in range(per_chunk):
            o = c * per_chunk + b

            @pl.when(o > 0)
            def _():
                dispatch_copy(o).wait_recv()

        ag_copy(c, 1, 0).start()
        ag_copy(c, 1, 1).start()
        d2d_copy(c, 0).start()

    def gather_hop(c, h):
        for way in (0, 1):
            ag_arrived(c, h, way)
            if h < hops:
                ag_copy(c, h + 1, way).start()
                d2d_copy(c, h if way == 0 else -h).start()
        if h == hops:
            d2d_copy(c, h).start()

    def feed_forward(c):
        @pl.when(c == 0)
        def _():
            for load in loads:
                load.wait()

            def gain_arrived(i, _):
                remote(gains.at[tp], gains.at[tp], gain_s.at[i], gain_r.at[i], ep, tp).wait_recv()
                return 0

            lax.fori_loop(1, n_tp, gain_arrived, 0)

        for q in range(nz):
            d2d_arrived(c, q)

        def norm(i, _):
            at = pl.ds(pl.multiple_of(c * rows + i * 16, 16), 16)
            vals = [x_all[j, at].astype(F32) for j in range(n_tp)]
            total = vals[0] * vals[0]
            for v in vals[1:]:
                total = total + v * v
            scale = lax.rsqrt(jnp.sum(total, axis=1, keepdims=True) / width + EPS)
            to = pl.ds(pl.multiple_of(i * 16, 16), 16)
            for j, v in enumerate(vals):
                x_norm[to, j * LANES:(j + 1) * LANES] = (v * scale * gains[j, 0:1, :]).astype(BF)
            return 0

        lax.fori_loop(0, rows // 16, norm, 0)
        tile = min(256, hid_pad)
        for at in range(0, hid_pad, tile):
            g = lax.dot_general(x_norm[...], gates[at:at + tile, :], NT, preferred_element_type=F32)
            u = lax.dot_general(x_norm[...], gates[hid_pad + at:hid_pad + at + tile, :], NT, preferred_element_type=F32)
            hidden[:, at:at + tile] = (g / (1.0 + jnp.exp(-g)) * u).astype(BF)

        for m in range(nz):
            p = jnp.dot(hidden[...], downs[:, m * 256:(m + 1) * 256], preferred_element_type=F32).astype(BF)
            part[c, 0, m] = p[:, :LANES]
            part[c, 1, m] = p[:, LANES:]
        peer_copy(c).start()

    def peer_copy(c):
        return remote(part.at[c, 1 - core], peer_part.at[c], pp_s.at[c], pp_r.at[c], ep, peer)

    def chip_sum(c, zd, at=0, count=None):
        sl = pl.ds(at, rows if count is None else count)
        return part[c, core, zd, sl, :].astype(F32) + peer_part[c, zd, sl, :].astype(F32)

    def rs_copy(c, s, way):
        at, count = (0, rows) if s > 1 else ((0, half) if way == 0 else (half, half))
        sl = pl.ds(at, count)
        return remote(
            ring_out.at[c, way, s - 1, sl], ring_in.at[c, way, s - 1, sl],
            rs_s.at[c, way, s - 1], rs_r.at[c, way, s - 1], ep, right if way == 0 else left,
        )

    def scatter_stage(c, s):
        if s == 1:
            peer_copy(c).wait_recv()
        for way in (0, 1):
            far = hops + 1 - s
            zd = lax.rem(z + far, nz) if way == 0 else lax.rem(z + nz - far, nz)
            if s == 1:
                at = 0 if way == 0 else half
                ring_out[c, way, 0, at:at + half, :] = chip_sum(c, zd, at, half).astype(BF)
            else:
                rs_copy(c, s - 1, way).wait_recv()
                for at in (0, half):
                    v = chip_sum(c, zd, at, half)
                    if s > 2 or (at == 0) == (way == 0):
                        v = v + ring_in[c, way, s - 2, at:at + half, :].astype(F32)
                    ring_out[c, way, s - 1, at:at + half, :] = v.astype(BF)
            rs_copy(c, s, way).start()

    def return_copy(o):
        return remote(
            results.at[block_rows(o)], returned.at[block_rows(o)], ret_s.at[o], ret_r.at[o], block_peer(o, -1), tp
        )

    def finish(c):
        for way in (0, 1):
            rs_copy(c, hops, way).wait_recv()
        for b in range(per_chunk):
            o = c * per_chunk + b
            at = b * cap
            v = chip_sum(c, z, at, cap)
            if hops > 1 or b * cap < half:
                v = v + ring_in[c, 0, hops - 1, at:at + cap, :].astype(F32)
            if hops > 1 or b * cap >= half:
                v = v + ring_in[c, 1, hops - 1, at:at + cap, :].astype(F32)
            v = v.astype(BF)

            @pl.when(o == 0)
            def _():
                returned[pl.ds(0, cap), :] = v

            @pl.when(o > 0)
            def _():
                results[block_rows(o), :] = v
                return_copy(o).start()

    def combine(c):
        for b in range(per_chunk):
            o = c * per_chunk + b

            @pl.when(o > 0)
            def _():
                return_copy(o).wait_recv()

        lane = lax.broadcasted_iota(jnp.int32, (toks, rows), 1).astype(F32) + (c * rows).astype(F32)
        values = returned[chunk_rows(c), :]
        for k in (0, 1):
            pick = jnp.where(lane == cols[:, k:k + 1], 1.0, 0.0).astype(BF)
            got = jnp.dot(pick, values, preferred_element_type=F32)

            @pl.when(c == 0)
            def _():
                sums[k] = got

            @pl.when(c > 0)
            def _():
                sums[k] = sums[k] + got

    stages = [gather_first]
    stages += [functools.partial(gather_hop, h=h) for h in range(1, hops + 1)]
    stages += [feed_forward]
    stages += [functools.partial(scatter_stage, s=s) for s in range(1, hops + 1)]
    stages += [finish, combine]

    def slot_step(t, _):
        for k, stage in enumerate(stages):
            c = t - k

            @pl.when((c >= 0) & (c < chunks))
            def _():
                stage(c)

        return 0

    lax.fori_loop(0, chunks + len(stages) - 1, slot_step, 0)

    both = cols[:, 2:3] * sums[0] + cols[:, 3:4] * sums[1]
    sums[0] = both
    square_own[...] = jnp.sum((both * both).T, axis=0, keepdims=True)

    def square_copy(i):
        return remote(square_own, squares.at[i], sq_s.at[i], sq_r.at[i], ep, lax.rem(tp + i, n_tp))

    def send_square(i, _):
        square_copy(i).start()
        return 0

    lax.fori_loop(1, n_tp, send_square, 0)

    def drain_block(o, _):
        dispatch_copy(o).wait_send()
        return_copy(o).wait_send()
        return 0

    lax.fori_loop(1, n_ep, drain_block, 0)

    def drain_chunk(c, _):
        for h in range(1, hops + 1):
            for way in (0, 1):
                ag_copy(c, h, way).wait_send()
                rs_copy(c, h, way).wait_send()
        for q in range(nz):
            d2d_copy(c, q).wait_send()
        peer_copy(c).wait_send()
        return 0

    lax.fori_loop(0, chunks, drain_chunk, 0)

    def drain_gain(i, _):
        remote(gains.at[tp], gains.at[tp], gain_s.at[i], gain_r.at[i], ep, tp).wait_send()
        return 0

    lax.fori_loop(1, n_tp, drain_gain, 0)

    total = square_own[...]
    for i in range(1, n_tp):
        square_copy(i).wait_recv()
        total = total + squares[i]
    scale = lax.rsqrt(total / width + EPS)
    scale = jnp.broadcast_to(scale, (8, toks)).T
    out[...] = (sums[0] * scale[:, 0:1] * post_gain[...].astype(F32)).astype(BF)

    def drain_square(i, _):
        square_copy(i).wait_send()
        return 0

    lax.fori_loop(1, n_tp, drain_square, 0)


def make(dims, toks, hid):
    ny, nx, nz, cap, per_chunk, width = dims
    n_ep, n_tp = ny * nx, nz * 2
    chunks, rows, hops = n_ep // per_chunk, cap * per_chunk, nz // 2
    hid_pad = -(-hid // 256) * 256 if hid > 128 else 128
    vmem = pl.BlockSpec(memory_space=pltpu.VMEM)
    hbm = pl.BlockSpec(memory_space=pl.ANY)
    dma = pltpu.SemaphoreType.DMA
    return pl.pallas_call(
        functools.partial(kernel, dims),
        out_shape=jax.ShapeDtypeStruct((toks, LANES), BF),
        in_specs=[vmem] * 5 + [hbm] * 3,
        out_specs=vmem,
        scratch_shapes=[
            pltpu.VMEM((2 * hid_pad, width), BF),
            pltpu.VMEM((hid_pad, width), BF),
            pltpu.VMEM((n_ep, toks), F32),
            pltpu.VMEM((toks, 8), F32),
            pltpu.VMEM((n_ep, cap, LANES), BF),
            pltpu.VMEM((n_tp, 8, LANES), F32),
            pltpu.VMEM((n_tp, n_ep * cap, LANES), BF),
            pltpu.VMEM((rows, width), BF),
            pltpu.VMEM((rows, hid_pad), BF),
            pltpu.VMEM((chunks, 2, nz, rows, LANES), BF),
            pltpu.VMEM((chunks, nz, rows, LANES), BF),
            pltpu.VMEM((chunks, 2, hops, rows, LANES), BF),
            pltpu.VMEM((chunks, 2, hops, rows, LANES), BF),
            pltpu.VMEM((n_ep * cap, LANES), BF),
            pltpu.VMEM((n_ep * cap, LANES), BF),
            pltpu.VMEM((2, toks, LANES), F32),
            pltpu.VMEM((n_tp, 1, toks), F32),
            pltpu.VMEM((1, toks), F32),
            dma((3,)),
            dma((n_tp,)), dma((n_tp,)),
            dma((n_ep,)), dma((n_ep,)),
            dma((chunks, 2, hops)), dma((chunks, 2, hops)),
            dma((chunks, nz)), dma((chunks, nz)),
            dma((chunks,)), dma((chunks,)),
            dma((chunks, 2, hops)), dma((chunks, 2, hops)),
            dma((n_ep,)), dma((n_ep,)),
            dma((n_tp,)), dma((n_tp,)),
        ],
        compiler_params=pltpu.CompilerParams(
            collective_id=0, has_side_effects=True, vmem_limit_bytes=66_000_000
        ),
        name="experts",
    )


def on_device(dims, tokens, pre_gain, ids, weights, gate_weight, up_weight, down_weight, post_gain):
    call = make(dims, tokens.shape[0], gate_weight.shape[2])
    return call(
        tokens, ids.T, weights.T, pre_gain[None], post_gain[None],
        gate_weight[0].T, up_weight[0].T, down_weight[0],
    )


def build(mesh, dims):
    placed = (
        P("ep", "tp"),
        P("tp"),
        P("ep", None),
        P("ep", None),
        P("ep", None, "tp"),
        P("ep", None, "tp"),
        P("ep", "tp", None),
        P("tp"),
    )
    return jax.shard_map(
        functools.partial(on_device, dims), mesh=mesh, in_specs=placed, out_specs=P("ep", "tp"), check_vma=False
    )


def solution(mesh):
    n_ep, n_tp = mesh.shape["ep"], mesh.shape["tp"]
    return build(mesh, (n_ep // NX, NX, n_tp // 2, 144, 2, 128 * n_tp))
```

```python
import functools

import jax
import jax.numpy as jnp
from jax import lax
from jax.experimental import pallas as pl
from jax.experimental.pallas import tpu as pltpu
from jax.sharding import PartitionSpec as P

BF, F32 = jnp.bfloat16, jnp.float32
MESH = pl.DeviceIdType.MESH
NX = 4
EPS = 1e-06
LANES = 128
TURNS = 4
FOLD_AT = 1
NT = (((1,), (1,)), ((), ()))


def near_first(i, n):
    return i if n < 4 else i + lax.div(i, 2) - 2 * lax.div(i, 3)


def kernel(
    dims,
    tokens, ids, weights, pre_gain, post_gain, gate_hbm, up_hbm, down_hbm,
    out,
    gates, downs, ranks, cols, outgoing, gains, x_all, x_norm, hidden,
    part, peer_part, ring_out, ring_in, results, returned, sums, squares, square_own,
    tok_near, near_sums, near_out, near_in, row_scale,
    w_sem, gain_s, gain_r, disp_s, disp_r, ag_s, ag_r, d2d_s, d2d_r,
    pp_s, pp_r, rs_s, rs_r, ret_s, ret_r, sq_s, sq_r,
    tn_s, tn_r, near_s, near_r, nret_s, nret_r, nx_s, nx_r,
):
    ny, nx, nz, cap, per_chunk, width, plain_in, plain_out = dims
    n_ep, n_tp = ny * nx, nz * 2
    chunks = n_ep // per_chunk
    rows = cap * per_chunk
    near_out_chunks = chunks - plain_out
    half = -(-rows // 32) * 16
    hops = nz // 2
    toks = tokens.shape[0]
    hid = gate_hbm.shape[0]
    hid_pad = downs.shape[0]

    ep, tp = lax.axis_index("ep"), lax.axis_index("tp")
    y, x = lax.div(ep, nx), lax.rem(ep, nx)
    z, core = lax.div(tp, 2), lax.rem(tp, 2)
    peer = z * 2 + 1 - core
    right = lax.rem(z + 1, nz) * 2 + core
    left = lax.rem(z + nz - 1, nz) * 2 + core

    def remote(src, dst, ssem, rsem, ep_to, tp_to):
        return pltpu.make_async_remote_copy(
            src_ref=src, dst_ref=dst, send_sem=ssem, recv_sem=rsem,
            device_id=(ep_to, tp_to), device_id_type=MESH,
        )

    def arrived(ref, sem):
        pltpu.make_async_copy(ref, ref, sem).wait()

    barrier = pltpu.get_barrier_semaphore()

    def greet_ep(i, _):
        pl.semaphore_signal(barrier, inc=1, device_id=(lax.rem(ep + i, n_ep), tp), device_id_type=MESH)
        return 0

    def greet_tp(i, _):
        pl.semaphore_signal(barrier, inc=1, device_id=(ep, lax.rem(tp + i, n_tp)), device_id_type=MESH)
        return 0

    lax.fori_loop(1, n_ep, greet_ep, 0)
    lax.fori_loop(1, n_tp, greet_tp, 0)

    loads = (
        pltpu.make_async_copy(gate_hbm, gates.at[pl.ds(0, hid)], w_sem.at[0]),
        pltpu.make_async_copy(up_hbm, gates.at[pl.ds(hid_pad, hid)], w_sem.at[1]),
        pltpu.make_async_copy(down_hbm, downs.at[pl.ds(0, hid)], w_sem.at[2]),
    )
    for load in loads:
        load.start()
    if hid_pad > hid:
        gates[pl.ds(hid, hid_pad - hid), :] = jnp.zeros((hid_pad - hid, width), BF)
        gates[pl.ds(hid_pad + hid, hid_pad - hid), :] = jnp.zeros((hid_pad - hid, width), BF)
        downs[pl.ds(hid, hid_pad - hid), :] = jnp.zeros((hid_pad - hid, width), BF)
    gains[tp] = pre_gain[...].astype(F32)

    o_i = lax.broadcasted_iota(jnp.int32, (n_ep, toks), 0)
    a_i, b_i = o_i // nx, o_i % nx

    def near_vec(i, n):
        return i if n < 4 else jnp.where(i == 2, 3, jnp.where(i == 3, 2, i))

    e_of = ((y + near_vec(a_i, ny)) % ny) * nx + (x + near_vec(b_i, nx)) % nx
    first = (ids[0:1, :] == e_of).astype(F32)
    second = (ids[1:2, :] == e_of).astype(F32)
    named = first + second
    named_bf = named.astype(BF)
    step = min(256, toks)
    for at in range(0, toks, step):
        before = lax.broadcasted_iota(jnp.int32, (toks, step), 0)
        after = lax.broadcasted_iota(jnp.int32, (toks, step), 1) + at
        upper = jnp.where(before < after, 1.0, 0.0).astype(BF)
        ranks[:, pl.ds(at, step)] = jnp.dot(named_bf, upper, preferred_element_type=F32)
    rank = ranks[...]
    slot = o_i.astype(F32) * float(cap) + rank
    slot0 = jnp.sum(first * slot, axis=0, keepdims=True)
    slot1 = jnp.sum(second * slot, axis=0, keepdims=True)
    ranks[...] = jnp.where(named > 0.0, rank, -1.0)
    r8 = lax.broadcasted_iota(jnp.int32, (8, toks), 0)
    table = jnp.where(r8 == 0, slot0, jnp.where(r8 == 1, slot1, jnp.where(r8 == 2, weights[0:1, :], weights[1:2, :])))
    cols[...] = table.T

    def block_peer(o, sign):
        dy = near_first(lax.div(o, nx), ny)
        dx = near_first(lax.rem(o, nx), nx)
        return lax.rem(y + ny + sign * dy, ny) * nx + lax.rem(x + nx + sign * dx, nx)

    def block_rows(o):
        return pl.ds(pl.multiple_of(o * cap, 16), cap)

    def dispatch_copy(o):
        return remote(
            outgoing.at[0, o], x_all.at[tp, block_rows(o)], disp_s, disp_r.at[o], block_peer(o, 1), tp
        )

    s_i = lax.broadcasted_iota(jnp.int32, (cap, toks), 0).astype(F32)

    def dispatch(o, _):
        pick = jnp.where(s_i == ranks[pl.ds(o, 1), :], 1.0, 0.0).astype(BF)
        picked = jnp.dot(pick, tokens[...], preferred_element_type=F32).astype(BF)

        @pl.when(o == 0)
        def _():
            x_all[tp, pl.ds(0, cap)] = picked

        @pl.when(o > 0)
        def _():
            outgoing[0, o] = picked

        return 0

    lax.fori_loop(0, n_ep, dispatch, 0)

    pl.semaphore_wait(barrier, n_ep - 1 + n_tp - 1)

    def send_gain(i, _):
        remote(gains.at[tp], gains.at[tp], gain_s, gain_r, ep, lax.rem(tp + i, n_tp)).start()
        return 0

    def token_copy(way):
        return remote(
            tokens, tok_near.at[way], tn_s.at[way], tn_r.at[way], ep, right if way == 0 else left
        )

    def send_block(o, _):
        dispatch_copy(o).start()
        return 0

    if plain_in < chunks:
        for way in (0, 1):
            token_copy(way).start()
    lax.fori_loop(1, n_ep, send_block, 0)
    lax.fori_loop(1, n_tp, send_gain, 0)

    def chunk_rows(c, at=0, count=None):
        return pl.ds(pl.multiple_of(c * rows + at, 16), rows if count is None else count)

    def slice_at(h):
        return lax.rem(z + 2 * nz - h, nz) * 2 + core

    def ag_copy(c, h, way):
        j = slice_at(h - 1 if way == 0 else 1 - h)
        at, count = (0, rows) if h < hops else ((0, half) if way == 0 else (half, rows - half))
        ref = x_all.at[j, chunk_rows(c, at, count)]
        return remote(ref, ref, ag_s.at[c], ag_r.at[lax.rem(c, TURNS), way, h - 1], ep, right if way == 0 else left)

    def ag_arrived(c, h, way):
        j = slice_at(h if way == 0 else -h)
        at, count = (0, rows) if h < hops else ((0, half) if way == 0 else (half, rows - half))
        ref = x_all.at[j, chunk_rows(c, at, count)]
        remote(ref, ref, ag_s.at[c], ag_r.at[lax.rem(c, TURNS), way, h - 1], ep, right).wait_recv()

    def d2d_copy(c, q):
        ref = x_all.at[slice_at(q), chunk_rows(c)]
        return remote(ref, ref, d2d_s, d2d_r.at[c], ep, peer)

    def near_copy(o, way):
        j = slice_at(1 if way == 0 else -1)
        return remote(
            outgoing.at[1 + way, o], x_all.at[j, block_rows(o)],
            near_s, near_r.at[lax.div(o, per_chunk)], block_peer(o, 1), tp,
        )

    def near_dispatch(c):
        @pl.when(c == plain_in)
        def _():
            for way in (0, 1):
                token_copy(way).wait_recv()

        for b in range(per_chunk):
            o = c * per_chunk + b
            pick = jnp.where(s_i == ranks[pl.ds(o, 1), :], 1.0, 0.0).astype(BF)
            both = jnp.concatenate([tok_near[0], tok_near[1]], axis=1)
            picked = jnp.dot(pick, both, preferred_element_type=F32).astype(BF)
            for way in (0, 1):
                outgoing[1 + way, o] = picked[:, way * LANES:(way + 1) * LANES]
                near_copy(o, way).start()

    def gather_first(c):
        for b in range(per_chunk):
            o = c * per_chunk + b

            @pl.when(o > 0)
            def _():
                dispatch_copy(o).wait_recv()

        @pl.when(c < plain_in)
        def _():
            ag_copy(c, 1, 0).start()
            ag_copy(c, 1, 1).start()

        d2d_copy(c, 0).start()

    def gather_hop(c, h):
        if h == 1:
            @pl.when(c >= plain_in)
            def _():
                arrived(x_all.at[pl.ds(0, 2), chunk_rows(c)], near_r.at[c])

        for way in (0, 1):
            if h > 1:
                ag_arrived(c, h, way)
            else:
                @pl.when(c < plain_in)
                def _():
                    ag_arrived(c, h, way)

            if h < hops:
                ag_copy(c, h + 1, way).start()
                d2d_copy(c, h if way == 0 else -h).start()
        if h == hops:
            d2d_copy(c, h).start()

    def fold_gain():
        for load in loads:
            load.wait()
        arrived(gains.at[pl.ds(1, n_tp - 1)], gain_r)
        gain = jnp.concatenate([gains[j] for j in range(n_tp)], axis=1)
        block = 64

        def fold(i, _):
            at = pl.ds(pl.multiple_of(i * block, block), block)
            gates[at, :] = (gates[at, :].astype(F32) * gain).astype(BF)
            return 0

        lax.fori_loop(0, 2 * hid_pad // block, fold, 0)

    def feed_forward(c):
        arrived(x_all.at[pl.ds(0, nz), chunk_rows(c)], d2d_r.at[c])

        def squares_of(i, _):
            at = pl.ds(pl.multiple_of(c * rows + i * 16, 16), 16)
            to = pl.ds(pl.multiple_of(i * 16, 16), 16)
            total = jnp.zeros((16, LANES), F32)
            for j in range(n_tp):
                raw = x_all[j, at]
                x_norm[to, j * LANES:(j + 1) * LANES] = raw
                v = raw.astype(F32)
                total = total + v * v
            mean = jnp.sum(total, axis=1, keepdims=True) / width
            row_scale[to, :] = jnp.broadcast_to(lax.rsqrt(mean + EPS), (16, LANES))
            return 0

        lax.fori_loop(0, rows // 16, squares_of, 0, unroll=3 if rows % 48 == 0 else 1)
        tile = min(256, hid_pad)
        for at in range(0, hid_pad, tile):
            g = lax.dot_general(x_norm[...], gates[at:at + tile, :], NT, preferred_element_type=F32)
            u = lax.dot_general(x_norm[...], gates[hid_pad + at:hid_pad + at + tile, :], NT, preferred_element_type=F32)
            scale = jnp.concatenate([row_scale[...]] * (tile // LANES), axis=1)
            g, u = g * scale, u * scale
            hidden[:, at:at + tile] = (g / (1.0 + jnp.exp(-g)) * u).astype(BF)

        for m in range(nz):
            p = jnp.dot(hidden[...], downs[:, m * 256:(m + 1) * 256], preferred_element_type=F32).astype(BF)
            part[c, 0, m] = p[:, :LANES]
            part[c, 1, m] = p[:, LANES:]
        peer_copy(c).start()

    def peer_copy(c):
        return remote(part.at[c, 1 - core], peer_part.at[c], pp_s, pp_r.at[lax.rem(c, TURNS)], ep, peer)

    def chip_sum(c, zd, at=0, count=None):
        sl = pl.ds(at, rows if count is None else count)
        return part[c, core, zd, sl, :].astype(F32) + peer_part[c, zd, sl, :].astype(F32)

    def rs_copy(c, s, way):
        at, count = (0, rows) if s > 1 else ((0, half) if way == 0 else (half, rows - half))
        sl = pl.ds(at, count)
        return remote(
            ring_out.at[c, way, s - 1, sl], ring_in.at[c, way, s - 1, sl],
            rs_s.at[c], rs_r.at[lax.rem(c, TURNS), way, s - 1], ep, right if way == 0 else left,
        )

    def scatter_stage(c, s):
        if s == 1:
            peer_copy(c).wait_recv()
        for way in (0, 1):
            far = hops + 1 - s
            zd = lax.rem(z + far, nz) if way == 0 else lax.rem(z + nz - far, nz)
            if s == 1:
                at = 0 if way == 0 else half
                count = half if way == 0 else rows - half
                ring_out[c, way, 0, at:at + count, :] = chip_sum(c, zd, at, count).astype(BF)
            else:
                rs_copy(c, s - 1, way).wait_recv()
                for at, count in ((0, half), (half, rows - half)):
                    v = chip_sum(c, zd, at, count)
                    if s > 2 or (at == 0) == (way == 0):
                        v = v + ring_in[c, way, s - 2, at:at + count, :].astype(F32)
                    ring_out[c, way, s - 1, at:at + count, :] = v.astype(BF)
            rs_copy(c, s, way).start()

    def return_copy(o):
        return remote(
            results.at[0, block_rows(o)], returned.at[0, block_rows(o)], ret_s, ret_r.at[o], block_peer(o, -1), tp
        )

    def near_return_copy(o, way):
        return remote(
            results.at[1 + way, block_rows(o)], returned.at[1 + way, block_rows(o)],
            nret_s, nret_r.at[lax.div(o, per_chunk)], block_peer(o, -1), tp,
        )

    def last_hop(c):
        @pl.when(c >= near_out_chunks)
        def _():
            scatter_stage(c, hops)

        @pl.when(c < near_out_chunks)
        def _():
            for way in (0, 1):
                rs_copy(c, hops - 1, way).wait_recv()
            for b in range(per_chunk):
                o = c * per_chunk + b
                at = b * cap
                own = chip_sum(c, z, at, cap).astype(BF)
                near = []
                for way in (0, 1):
                    zd = lax.rem(z + 1, nz) if way == 0 else lax.rem(z + nz - 1, nz)
                    v = chip_sum(c, zd, at, cap) + ring_in[c, way, hops - 2, at:at + cap, :].astype(F32)
                    near.append(v.astype(BF))

                @pl.when(o == 0)
                def _():
                    returned[0, pl.ds(0, cap), :] = own
                    for way in (0, 1):
                        returned[1 + way, pl.ds(0, cap), :] = near[way]

                @pl.when(o > 0)
                def _():
                    results[0, block_rows(o), :] = own
                    return_copy(o).start()
                    for way in (0, 1):
                        results[1 + way, block_rows(o), :] = near[way]
                        near_return_copy(o, way).start()

    def finish(c):
        @pl.when(c < near_out_chunks)
        def _():
            combine(c, True)

        @pl.when(c >= near_out_chunks)
        def _():
            for way in (0, 1):
                rs_copy(c, hops, way).wait_recv()
            for b in range(per_chunk):
                o = c * per_chunk + b
                at = b * cap
                v = chip_sum(c, z, at, cap)
                for way in (0, 1):
                    v = v + ring_in[c, way, hops - 1, at:at + cap, :].astype(F32)
                v = v.astype(BF)

                @pl.when(o == 0)
                def _():
                    returned[0, pl.ds(0, cap), :] = v

                @pl.when(o > 0)
                def _():
                    results[0, block_rows(o), :] = v
                    return_copy(o).start()

    def near_sum_copy(way):
        return remote(
            near_out.at[way], near_in.at[way], nx_s.at[way], nx_r.at[way], ep, right if way == 0 else left
        )

    def combine(c, near):
        for b in range(per_chunk):
            o = c * per_chunk + b

            @pl.when(o > 0)
            def _():
                return_copy(o).wait_recv()

        lane = lax.broadcasted_iota(jnp.int32, (toks, rows), 1).astype(F32) + (c * rows).astype(F32)
        values = returned[0, chunk_rows(c), :]
        if near:
            @pl.when(c > 0)
            def _():
                arrived(x_all.at[pl.ds(0, 2), chunk_rows(c)], nret_r.at[c])

            @pl.when(c == 0)
            def _():
                if per_chunk > 1:
                    arrived(x_all.at[pl.ds(0, 2), pl.ds(0, rows - cap)], nret_r.at[c])

            values = jnp.concatenate([values, returned[1, chunk_rows(c), :], returned[2, chunk_rows(c), :]], axis=1)
        for k in (0, 1):
            pick = jnp.where(lane == cols[:, k:k + 1], 1.0, 0.0).astype(BF)
            got = jnp.dot(pick, values, preferred_element_type=F32)

            @pl.when(c == 0)
            def _():
                sums[k] = got[:, :LANES]
                if near:
                    near_sums[k] = got[:, LANES:]

            @pl.when(c > 0)
            def _():
                sums[k] = sums[k] + got[:, :LANES]
                if near:
                    near_sums[k] = near_sums[k] + got[:, LANES:]

        if near:
            @pl.when(c == near_out_chunks - 1)
            def _():
                total = cols[:, 2:3] * near_sums[0] + cols[:, 3:4] * near_sums[1]
                for way in (0, 1):
                    near_out[way] = total[:, way * LANES:(way + 1) * LANES].astype(BF)
                    near_sum_copy(way).start()

    def last_combine(c):
        @pl.when(c >= near_out_chunks)
        def _():
            combine(c, False)

    stages = [(gather_first, 0)]
    if plain_in < chunks:
        stages += [(near_dispatch, -1)]
    stages += [(functools.partial(gather_hop, h=h), h) for h in range(1, hops + 1)]
    stages += [(feed_forward, hops + 1)]
    stages += [(functools.partial(scatter_stage, s=s), hops + 1 + s) for s in range(1, hops)]
    stages += [(last_hop, 2 * hops + 1), (finish, 2 * hops + 2), (last_combine, 2 * hops + 3)]

    def slot_step(t, _):
        @pl.when(t == FOLD_AT)
        def _():
            fold_gain()

        for stage, first_slot in stages:
            c = t - first_slot
            low = plain_in if stage is near_dispatch else 0

            @pl.when((c >= low) & (c < chunks))
            def _():
                stage(c)

        return 0

    lax.fori_loop(0, chunks + 2 * hops + 3, slot_step, 0)

    both = cols[:, 2:3] * sums[0] + cols[:, 3:4] * sums[1]
    if near_out_chunks:
        for way in (0, 1):
            near_sum_copy(way).wait_recv()
            both = both + near_in[way].astype(F32)
    sums[0] = both
    square_own[...] = jnp.sum((both * both).T, axis=0, keepdims=True)

    def square_copy(i):
        return remote(square_own, squares.at[i], sq_s, sq_r, ep, lax.rem(tp + i, n_tp))

    def send_square(i, _):
        square_copy(i).start()
        return 0

    lax.fori_loop(1, n_tp, send_square, 0)

    arrived(gains.at[pl.ds(1, n_tp - 1)], gain_s)
    arrived(outgoing.at[0, pl.ds(1, n_ep - 1)], disp_s)
    arrived(results.at[0, pl.ds(cap, (n_ep - 1) * cap)], ret_s)
    arrived(x_all.at[pl.ds(0, nz)], d2d_s)
    arrived(x_all.at[pl.ds(0, nz)], pp_s)
    for c in range(chunks):
        arrived(part.at[c, 0, pl.ds(0, nz - 1 if c < plain_in else nz - 3)], ag_s.at[c])
        arrived(part.at[c, 0, pl.ds(0, nz - 3 if c < near_out_chunks else nz - 1)], rs_s.at[c])
    first_near = plain_in * per_chunk
    if first_near < n_ep:
        arrived(outgoing.at[pl.ds(1, 2), pl.ds(first_near, n_ep - first_near)], near_s)
    last_near = near_out_chunks * per_chunk
    if last_near > 1:
        arrived(results.at[pl.ds(1, 2), pl.ds(cap, (last_near - 1) * cap)], nret_s)
    for way in (0, 1):
        if plain_in < chunks:
            token_copy(way).wait_send()
        if near_out_chunks:
            near_sum_copy(way).wait_send()

    total = square_own[...]
    arrived(squares.at[pl.ds(1, n_tp - 1)], sq_r)
    for i in range(1, n_tp):
        total = total + squares[i]
    scale = lax.rsqrt(total / width + EPS)
    scale = jnp.broadcast_to(scale, (8, toks)).T
    out[...] = (sums[0] * scale[:, 0:1] * post_gain[...].astype(F32)).astype(BF)

    arrived(squares.at[pl.ds(1, n_tp - 1)], sq_s)


def make(dims, toks, hid):
    ny, nx, nz, cap, per_chunk, width, _, _ = dims
    n_ep, n_tp = ny * nx, nz * 2
    chunks, rows, hops = n_ep // per_chunk, cap * per_chunk, nz // 2
    hid_pad = -(-hid // 256) * 256 if hid > 128 else 128
    vmem = pl.BlockSpec(memory_space=pltpu.VMEM)
    hbm = pl.BlockSpec(memory_space=pl.ANY)
    dma = pltpu.SemaphoreType.DMA
    return pl.pallas_call(
        functools.partial(kernel, dims),
        out_shape=jax.ShapeDtypeStruct((toks, LANES), BF),
        in_specs=[vmem] * 5 + [hbm] * 3,
        out_specs=vmem,
        scratch_shapes=[
            pltpu.VMEM((2 * hid_pad, width), BF),
            pltpu.VMEM((hid_pad, width), BF),
            pltpu.VMEM((n_ep, toks), F32),
            pltpu.VMEM((toks, 8), F32),
            pltpu.VMEM((3, n_ep, cap, LANES), BF),
            pltpu.VMEM((n_tp, 1, LANES), F32),
            pltpu.VMEM((n_tp, n_ep * cap, LANES), BF),
            pltpu.VMEM((rows, width), BF),
            pltpu.VMEM((rows, hid_pad), BF),
            pltpu.VMEM((chunks, 2, nz, rows, LANES), BF),
            pltpu.VMEM((chunks, nz, rows, LANES), BF),
            pltpu.VMEM((chunks, 2, hops, rows, LANES), BF),
            pltpu.VMEM((chunks, 2, hops, rows, LANES), BF),
            pltpu.VMEM((3, n_ep * cap, LANES), BF),
            pltpu.VMEM((3, n_ep * cap, LANES), BF),
            pltpu.VMEM((2, toks, LANES), F32),
            pltpu.VMEM((n_tp, 1, toks), F32),
            pltpu.VMEM((1, toks), F32),
            pltpu.VMEM((2, toks, LANES), BF),
            pltpu.VMEM((2, toks, 2 * LANES), F32),
            pltpu.VMEM((2, toks, LANES), BF),
            pltpu.VMEM((2, toks, LANES), BF),
            pltpu.VMEM((rows, LANES), F32),
            dma((3,)),
            dma, dma,
            dma, dma((n_ep,)),
            dma((chunks,)), dma((TURNS, 2, hops)), dma, dma((chunks,)),
            dma, dma((TURNS,)),
            dma((chunks,)), dma((TURNS, 2, hops)),
            dma, dma((n_ep,)),
            dma, dma,
            dma((2,)), dma((2,)),
            dma, dma((chunks,)),
            dma, dma((chunks,)),
            dma((2,)), dma((2,)),
        ],
        compiler_params=pltpu.CompilerParams(
            collective_id=0, has_side_effects=True, vmem_limit_bytes=66_000_000
        ),
        name="experts",
    )


def on_device(dims, tokens, pre_gain, ids, weights, gate_weight, up_weight, down_weight, post_gain):
    call = make(dims, tokens.shape[0], gate_weight.shape[2])
    return call(
        tokens, ids.T, weights.T, pre_gain[None], post_gain[None],
        gate_weight[0].T, up_weight[0].T, down_weight[0],
    )


def build(mesh, dims):
    placed = (
        P("ep", "tp"),
        P("tp"),
        P("ep", None),
        P("ep", None),
        P("ep", None, "tp"),
        P("ep", None, "tp"),
        P("ep", "tp", None),
        P("tp"),
    )
    return jax.shard_map(
        functools.partial(on_device, dims), mesh=mesh, in_specs=placed, out_specs=P("ep", "tp"), check_vma=False
    )


def solution(mesh):
    n_ep, n_tp = mesh.shape["ep"], mesh.shape["tp"]
    return build(mesh, (n_ep // NX, NX, n_tp // 2, 144, 2, 128 * n_tp, 8, 8))
```

```python
import functools

import jax
import jax.numpy as jnp
from jax import lax
from jax.experimental import pallas as pl
from jax.experimental.pallas import tpu as pltpu
from jax.sharding import PartitionSpec as P

BF, F32 = jnp.bfloat16, jnp.float32
MESH = pl.DeviceIdType.MESH
NX = 4
EPS = 1e-06
LANES = 128
TURNS = 4
FOLD_AT = 1
NT = (((1,), (1,)), ((), ()))


def near_first(i, n):
    return i if n < 4 else i + lax.div(i, 2) - 2 * lax.div(i, 3)


def kernel(
    dims,
    tokens, ids, weights, pre_gain, post_gain, gate_hbm, up_hbm, down_hbm,
    out,
    gates, downs, ranks, cols, outgoing, gains, x_all, x_norm, hidden,
    part, peer_part, ring_out, ring_in, results, returned, sums, squares, square_own,
    tok_near, near_sums, near_out, near_in, row_scale,
    w_sem, gain_s, gain_r, disp_s, disp_r, ag_s, ag_r, d2d_s, d2d_r,
    pp_s, pp_r, rs_s, rs_r, ret_s, ret_r, sq_s, sq_r,
    tn_s, tn_r, near_s, near_r, nret_s, nret_r, nx_s, nx_r,
):
    ny, nx, nz, cap, per_chunk, width, plain_in, plain_out = dims
    n_ep, n_tp = ny * nx, nz * 2
    chunks = n_ep // per_chunk
    rows = cap * per_chunk
    near_out_chunks = chunks - plain_out
    half = -(-rows // 32) * 16
    hops = nz // 2
    toks = tokens.shape[0]
    hid = gate_hbm.shape[0]
    hid_pad = downs.shape[0]

    ep, tp = lax.axis_index("ep"), lax.axis_index("tp")
    y, x = lax.div(ep, nx), lax.rem(ep, nx)
    z, core = lax.div(tp, 2), lax.rem(tp, 2)
    peer = z * 2 + 1 - core
    right = lax.rem(z + 1, nz) * 2 + core
    left = lax.rem(z + nz - 1, nz) * 2 + core

    def remote(src, dst, ssem, rsem, ep_to, tp_to):
        return pltpu.make_async_remote_copy(
            src_ref=src, dst_ref=dst, send_sem=ssem, recv_sem=rsem,
            device_id=(ep_to, tp_to), device_id_type=MESH,
        )

    def arrived(ref, sem):
        pltpu.make_async_copy(ref, ref, sem).wait()

    barrier = pltpu.get_barrier_semaphore()

    def greet_ep(i, _):
        pl.semaphore_signal(barrier, inc=1, device_id=(lax.rem(ep + i, n_ep), tp), device_id_type=MESH)
        return 0

    def greet_tp(i, _):
        pl.semaphore_signal(barrier, inc=1, device_id=(ep, lax.rem(tp + i, n_tp)), device_id_type=MESH)
        return 0

    lax.fori_loop(1, n_ep, greet_ep, 0)
    lax.fori_loop(1, n_tp, greet_tp, 0)

    loads = (
        pltpu.make_async_copy(gate_hbm, gates.at[pl.ds(0, hid)], w_sem.at[0]),
        pltpu.make_async_copy(up_hbm, gates.at[pl.ds(hid_pad, hid)], w_sem.at[1]),
        pltpu.make_async_copy(down_hbm, downs.at[pl.ds(0, hid)], w_sem.at[2]),
    )
    for load in loads:
        load.start()
    if hid_pad > hid:
        gates[pl.ds(hid, hid_pad - hid), :] = jnp.zeros((hid_pad - hid, width), BF)
        gates[pl.ds(hid_pad + hid, hid_pad - hid), :] = jnp.zeros((hid_pad - hid, width), BF)
        downs[pl.ds(hid, hid_pad - hid), :] = jnp.zeros((hid_pad - hid, width), BF)
    gains[tp] = pre_gain[...].astype(F32)

    o_i = lax.broadcasted_iota(jnp.int32, (n_ep, toks), 0)
    a_i, b_i = o_i // nx, o_i % nx

    def near_vec(i, n):
        return i if n < 4 else jnp.where(i == 2, 3, jnp.where(i == 3, 2, i))

    e_of = ((y + near_vec(a_i, ny)) % ny) * nx + (x + near_vec(b_i, nx)) % nx
    first = (ids[0:1, :] == e_of).astype(F32)
    second = (ids[1:2, :] == e_of).astype(F32)
    named = first + second
    named_bf = named.astype(BF)
    step = min(256, toks)
    for at in range(0, toks, step):
        before = lax.broadcasted_iota(jnp.int32, (toks, step), 0)
        after = lax.broadcasted_iota(jnp.int32, (toks, step), 1) + at
        upper = jnp.where(before < after, 1.0, 0.0).astype(BF)
        ranks[:, pl.ds(at, step)] = jnp.dot(named_bf, upper, preferred_element_type=F32)
    rank = ranks[...]
    slot = o_i.astype(F32) * float(cap) + rank
    slot0 = jnp.sum(first * slot, axis=0, keepdims=True)
    slot1 = jnp.sum(second * slot, axis=0, keepdims=True)
    ranks[...] = jnp.where(named > 0.0, rank, -1.0)
    r8 = lax.broadcasted_iota(jnp.int32, (8, toks), 0)
    table = jnp.where(r8 == 0, slot0, jnp.where(r8 == 1, slot1, jnp.where(r8 == 2, weights[0:1, :], weights[1:2, :])))
    cols[...] = table.T

    def block_peer(o, sign):
        dy = near_first(lax.div(o, nx), ny)
        dx = near_first(lax.rem(o, nx), nx)
        return lax.rem(y + ny + sign * dy, ny) * nx + lax.rem(x + nx + sign * dx, nx)

    def block_rows(o):
        return pl.ds(pl.multiple_of(o * cap, 16), cap)

    def dispatch_copy(o):
        return remote(
            outgoing.at[0, o], x_all.at[tp, block_rows(o)], disp_s, disp_r.at[o], block_peer(o, 1), tp
        )

    s_i = lax.broadcasted_iota(jnp.int32, (cap, toks), 0).astype(F32)

    def dispatch(o, _):
        pick = jnp.where(s_i == ranks[pl.ds(o, 1), :], 1.0, 0.0).astype(BF)
        picked = jnp.dot(pick, tokens[...], preferred_element_type=F32).astype(BF)

        @pl.when(o == 0)
        def _():
            x_all[tp, pl.ds(0, cap)] = picked

        @pl.when(o > 0)
        def _():
            outgoing[0, o] = picked

        return 0

    lax.fori_loop(0, n_ep, dispatch, 0)

    pl.semaphore_wait(barrier, n_ep - 1 + n_tp - 1)

    def send_gain(i, _):
        remote(gains.at[tp], gains.at[tp], gain_s, gain_r, ep, lax.rem(tp + i, n_tp)).start()
        return 0

    def token_copy(way):
        return remote(
            tokens, tok_near.at[way], tn_s.at[way], tn_r.at[way], ep, right if way == 0 else left
        )

    def send_block(o, _):
        dispatch_copy(o).start()
        return 0

    if plain_in < chunks:
        for way in (0, 1):
            token_copy(way).start()
    lax.fori_loop(1, n_ep, send_block, 0)
    lax.fori_loop(1, n_tp, send_gain, 0)

    def chunk_rows(c, at=0, count=None):
        return pl.ds(pl.multiple_of(c * rows + at, 16), rows if count is None else count)

    def slice_at(h):
        return lax.rem(z + 2 * nz - h, nz) * 2 + core

    def sub_rows(sub):
        return (0, half) if sub == 0 else (half, rows - half)

    def subs_of(h, way):
        return (0, 1) if h < hops else (way,)

    def ag_copy(c, h, way, sub):
        ref = x_all.at[slice_at(h - 1 if way == 0 else 1 - h), chunk_rows(c, *sub_rows(sub))]
        return remote(
            ref, ref, ag_s.at[c], ag_r.at[lax.rem(c, TURNS), way, h - 1, sub], ep, right if way == 0 else left
        )

    def ag_arrived(c, h, way, sub):
        ref = x_all.at[slice_at(h if way == 0 else -h), chunk_rows(c, *sub_rows(sub))]
        remote(ref, ref, ag_s.at[c], ag_r.at[lax.rem(c, TURNS), way, h - 1, sub], ep, right).wait_recv()

    def d2d_copy(c, q):
        ref = x_all.at[slice_at(q), chunk_rows(c)]
        return remote(ref, ref, d2d_s, d2d_r.at[c], ep, peer)

    def near_copy(o, way):
        j = slice_at(1 if way == 0 else -1)
        return remote(
            outgoing.at[1 + way, o], x_all.at[j, block_rows(o)],
            near_s, near_r.at[lax.div(o, per_chunk)], block_peer(o, 1), tp,
        )

    def near_dispatch(c):
        @pl.when(c == plain_in)
        def _():
            for way in (0, 1):
                token_copy(way).wait_recv()

        for b in range(per_chunk):
            o = c * per_chunk + b
            pick = jnp.where(s_i == ranks[pl.ds(o, 1), :], 1.0, 0.0).astype(BF)
            both = jnp.concatenate([tok_near[0], tok_near[1]], axis=1)
            picked = jnp.dot(pick, both, preferred_element_type=F32).astype(BF)
            for way in (0, 1):
                outgoing[1 + way, o] = picked[:, way * LANES:(way + 1) * LANES]
                near_copy(o, way).start()

    def gather_first(c):
        for b in range(per_chunk):
            o = c * per_chunk + b

            @pl.when(o > 0)
            def _():
                dispatch_copy(o).wait_recv()

            if (b + 1) * cap in (half, rows):
                sub = 0 if (b + 1) * cap == half else 1

                @pl.when(c < plain_in)
                def _():
                    for way in (0, 1):
                        for piece in ((0, 1) if per_chunk == 1 else (sub,)):
                            ag_copy(c, 1, way, piece).start()


        d2d_copy(c, 0).start()

    def gather_hop(c, h):
        if h == 1:
            @pl.when(c >= plain_in)
            def _():
                arrived(x_all.at[pl.ds(0, 2), chunk_rows(c)], near_r.at[c])

        for sub in (0, 1):
            for way in (0, 1):
                if sub not in subs_of(h, way):
                    continue
                if h > 1:
                    ag_arrived(c, h, way, sub)
                else:
                    @pl.when(c < plain_in)
                    def _():
                        ag_arrived(c, h, way, sub)

                if h < hops and sub in subs_of(h + 1, way):
                    ag_copy(c, h + 1, way, sub).start()
                if h < hops and sub == 1:
                    d2d_copy(c, h if way == 0 else -h).start()

        if h == hops:
            d2d_copy(c, h).start()

    def fold_gain():
        for load in loads:
            load.wait()
        arrived(gains.at[pl.ds(1, n_tp - 1)], gain_r)
        gain = jnp.concatenate([gains[j] for j in range(n_tp)], axis=1)
        block = 64

        def fold(i, _):
            at = pl.ds(pl.multiple_of(i * block, block), block)
            gates[at, :] = (gates[at, :].astype(F32) * gain).astype(BF)
            return 0

        lax.fori_loop(0, 2 * hid_pad // block, fold, 0)

    def feed_forward(c):
        arrived(x_all.at[pl.ds(0, nz), chunk_rows(c)], d2d_r.at[c])

        def squares_of(i, _):
            at = pl.ds(pl.multiple_of(c * rows + i * 16, 16), 16)
            to = pl.ds(pl.multiple_of(i * 16, 16), 16)
            total = jnp.zeros((16, LANES), F32)
            for j in range(n_tp):
                raw = x_all[j, at]
                x_norm[to, j * LANES:(j + 1) * LANES] = raw
                v = raw.astype(F32)
                total = total + v * v
            mean = jnp.sum(total, axis=1, keepdims=True) / width
            row_scale[to, :] = jnp.broadcast_to(lax.rsqrt(mean + EPS), (16, LANES))
            return 0

        lax.fori_loop(0, rows // 16, squares_of, 0, unroll=3 if rows % 48 == 0 else 1)
    tile = min(256, hid_pad)

    def project(c, at):
        g = lax.dot_general(x_norm[...], gates[at:at + tile, :], NT, preferred_element_type=F32)
        u = lax.dot_general(x_norm[...], gates[hid_pad + at:hid_pad + at + tile, :], NT, preferred_element_type=F32)
        scale = jnp.concatenate([row_scale[...]] * (tile // LANES), axis=1)
        g, u = g * scale, u * scale
        hidden[:, at:at + tile] = (g / (1.0 + jnp.exp(-g)) * u).astype(BF)

    def project_down(c):
        for m in range(nz):
            p = jnp.dot(hidden[...], downs[:, m * 256:(m + 1) * 256], preferred_element_type=F32).astype(BF)
            part[c, 0, m] = p[:, :LANES]
            part[c, 1, m] = p[:, LANES:]
        peer_copy(c).start()

    def peer_copy(c):
        return remote(part.at[c, 1 - core], peer_part.at[c], pp_s, pp_r.at[lax.rem(c, TURNS)], ep, peer)

    def chip_sum(c, zd, at=0, count=None):
        sl = pl.ds(at, rows if count is None else count)
        return part[c, core, zd, sl, :].astype(F32) + peer_part[c, zd, sl, :].astype(F32)

    def rs_subs(s, way):
        return (0, 1) if s > 1 else (way,)

    def rs_copy(c, s, way, sub):
        sl = pl.ds(*sub_rows(sub))
        return remote(
            ring_out.at[c, way, s - 1, sl], ring_in.at[c, way, s - 1, sl],
            rs_s.at[c], rs_r.at[lax.rem(c, TURNS), way, s - 1, sub], ep, right if way == 0 else left,
        )

    def scatter_stage(c, s):
        if s == 1:
            peer_copy(c).wait_recv()
        far = hops + 1 - s
        for sub in (0, 1):
            at, count = sub_rows(sub)
            for way in (0, 1):
                if sub not in rs_subs(s, way):
                    continue
                zd = lax.rem(z + far, nz) if way == 0 else lax.rem(z + nz - far, nz)
                v = chip_sum(c, zd, at, count)
                if s > 1 and sub in rs_subs(s - 1, way):
                    rs_copy(c, s - 1, way, sub).wait_recv()
                    v = v + ring_in[c, way, s - 2, at:at + count, :].astype(F32)
                ring_out[c, way, s - 1, at:at + count, :] = v.astype(BF)
                rs_copy(c, s, way, sub).start()

    def stage_arrived(c, s):
        for sub in (0, 1):
            for way in (0, 1):
                if sub in rs_subs(s, way):
                    rs_copy(c, s, way, sub).wait_recv()

    def return_copy(o):
        return remote(
            results.at[0, block_rows(o)], returned.at[0, block_rows(o)], ret_s, ret_r.at[o], block_peer(o, -1), tp
        )

    def near_return_copy(o, way):
        return remote(
            results.at[1 + way, block_rows(o)], returned.at[1 + way, block_rows(o)],
            nret_s, nret_r.at[lax.div(o, per_chunk)], block_peer(o, -1), tp,
        )

    def last_hop(c):
        @pl.when(c >= near_out_chunks)
        def _():
            scatter_stage(c, hops)

        @pl.when(c < near_out_chunks)
        def _():
            stage_arrived(c, hops - 1)
            for b in range(per_chunk):
                o = c * per_chunk + b
                at = b * cap
                own = chip_sum(c, z, at, cap).astype(BF)
                near = []
                for way in (0, 1):
                    zd = lax.rem(z + 1, nz) if way == 0 else lax.rem(z + nz - 1, nz)
                    v = chip_sum(c, zd, at, cap) + ring_in[c, way, hops - 2, at:at + cap, :].astype(F32)
                    near.append(v.astype(BF))

                @pl.when(o == 0)
                def _():
                    returned[0, pl.ds(0, cap), :] = own
                    for way in (0, 1):
                        returned[1 + way, pl.ds(0, cap), :] = near[way]

                @pl.when(o > 0)
                def _():
                    results[0, block_rows(o), :] = own
                    return_copy(o).start()
                    for way in (0, 1):
                        results[1 + way, block_rows(o), :] = near[way]
                        near_return_copy(o, way).start()

    def finish(c):
        @pl.when(c < near_out_chunks)
        def _():
            combine(c, True)

        @pl.when(c >= near_out_chunks)
        def _():
            stage_arrived(c, hops)
            for b in range(per_chunk):
                o = c * per_chunk + b
                at = b * cap
                v = chip_sum(c, z, at, cap)
                for way in (0, 1):
                    v = v + ring_in[c, way, hops - 1, at:at + cap, :].astype(F32)
                v = v.astype(BF)

                @pl.when(o == 0)
                def _():
                    returned[0, pl.ds(0, cap), :] = v

                @pl.when(o > 0)
                def _():
                    results[0, block_rows(o), :] = v
                    return_copy(o).start()

    def near_sum_copy(way):
        return remote(
            near_out.at[way], near_in.at[way], nx_s.at[way], nx_r.at[way], ep, right if way == 0 else left
        )

    def combine(c, near):
        for b in range(per_chunk):
            o = c * per_chunk + b

            @pl.when(o > 0)
            def _():
                return_copy(o).wait_recv()

        lane = lax.broadcasted_iota(jnp.int32, (toks, rows), 1).astype(F32) + (c * rows).astype(F32)
        values = returned[0, chunk_rows(c), :]
        if near:
            @pl.when(c > 0)
            def _():
                arrived(x_all.at[pl.ds(0, 2), chunk_rows(c)], nret_r.at[c])

            @pl.when(c == 0)
            def _():
                if per_chunk > 1:
                    arrived(x_all.at[pl.ds(0, 2), pl.ds(0, rows - cap)], nret_r.at[c])

            values = jnp.concatenate([values, returned[1, chunk_rows(c), :], returned[2, chunk_rows(c), :]], axis=1)
        for k in (0, 1):
            pick = jnp.where(lane == cols[:, k:k + 1], 1.0, 0.0).astype(BF)
            got = jnp.dot(pick, values, preferred_element_type=F32)

            @pl.when(c == 0)
            def _():
                sums[k] = got[:, :LANES]
                if near:
                    near_sums[k] = got[:, LANES:]

            @pl.when(c > 0)
            def _():
                sums[k] = sums[k] + got[:, :LANES]
                if near:
                    near_sums[k] = near_sums[k] + got[:, LANES:]

        if near:
            @pl.when(c == near_out_chunks - 1)
            def _():
                total = cols[:, 2:3] * near_sums[0] + cols[:, 3:4] * near_sums[1]
                for way in (0, 1):
                    near_out[way] = total[:, way * LANES:(way + 1) * LANES].astype(BF)
                    near_sum_copy(way).start()

    def last_combine(c):
        @pl.when(c >= near_out_chunks)
        def _():
            combine(c, False)

    stages = [(gather_first, 0)]
    if plain_in < chunks:
        stages += [(near_dispatch, -1)]
    hop = [(functools.partial(gather_hop, h=h), h) for h in range(1, hops + 1)]
    forward = [feed_forward] + [functools.partial(project, at=at) for at in range(0, hid_pad, tile)] + [project_down]
    forward = [(part_of, hops + 1) for part_of in forward]
    while hop or forward:
        stages += hop[:1] + forward[:1]
        hop, forward = hop[1:], forward[1:]
    stages += [(functools.partial(scatter_stage, s=s), hops + 1 + s) for s in range(1, hops)]
    stages += [(last_hop, 2 * hops + 1), (finish, 2 * hops + 2), (last_combine, 2 * hops + 3)]

    def slot_step(t, _):
        @pl.when(t == FOLD_AT)
        def _():
            fold_gain()

        for stage, first_slot in stages:
            c = t - first_slot
            low = plain_in if stage is near_dispatch else 0

            @pl.when((c >= low) & (c < chunks))
            def _():
                stage(c)

        return 0

    lax.fori_loop(0, chunks + 2 * hops + 3, slot_step, 0)

    both = cols[:, 2:3] * sums[0] + cols[:, 3:4] * sums[1]
    if near_out_chunks:
        for way in (0, 1):
            near_sum_copy(way).wait_recv()
            both = both + near_in[way].astype(F32)
    sums[0] = both
    square_own[...] = jnp.sum((both * both).T, axis=0, keepdims=True)

    def square_copy(i):
        return remote(square_own, squares.at[i], sq_s, sq_r, ep, lax.rem(tp + i, n_tp))

    def send_square(i, _):
        square_copy(i).start()
        return 0

    lax.fori_loop(1, n_tp, send_square, 0)

    arrived(gains.at[pl.ds(1, n_tp - 1)], gain_s)
    arrived(outgoing.at[0, pl.ds(1, n_ep - 1)], disp_s)
    arrived(results.at[0, pl.ds(cap, (n_ep - 1) * cap)], ret_s)
    arrived(x_all.at[pl.ds(0, nz)], d2d_s)
    arrived(x_all.at[pl.ds(0, nz)], pp_s)
    for c in range(chunks):
        arrived(part.at[c, 0, pl.ds(0, nz - 1 if c < plain_in else nz - 3)], ag_s.at[c])
        arrived(part.at[c, 0, pl.ds(0, nz - 3 if c < near_out_chunks else nz - 1)], rs_s.at[c])
    first_near = plain_in * per_chunk
    if first_near < n_ep:
        arrived(outgoing.at[pl.ds(1, 2), pl.ds(first_near, n_ep - first_near)], near_s)
    last_near = near_out_chunks * per_chunk
    if last_near > 1:
        arrived(results.at[pl.ds(1, 2), pl.ds(cap, (last_near - 1) * cap)], nret_s)
    for way in (0, 1):
        if plain_in < chunks:
            token_copy(way).wait_send()
        if near_out_chunks:
            near_sum_copy(way).wait_send()

    total = square_own[...]
    arrived(squares.at[pl.ds(1, n_tp - 1)], sq_r)
    for i in range(1, n_tp):
        total = total + squares[i]
    scale = lax.rsqrt(total / width + EPS)
    scale = jnp.broadcast_to(scale, (8, toks)).T
    out[...] = (sums[0] * scale[:, 0:1] * post_gain[...].astype(F32)).astype(BF)

    arrived(squares.at[pl.ds(1, n_tp - 1)], sq_s)


def make(dims, toks, hid):
    ny, nx, nz, cap, per_chunk, width, _, _ = dims
    n_ep, n_tp = ny * nx, nz * 2
    chunks, rows, hops = n_ep // per_chunk, cap * per_chunk, nz // 2
    hid_pad = -(-hid // 256) * 256 if hid > 128 else 128
    vmem = pl.BlockSpec(memory_space=pltpu.VMEM)
    hbm = pl.BlockSpec(memory_space=pl.ANY)
    dma = pltpu.SemaphoreType.DMA
    return pl.pallas_call(
        functools.partial(kernel, dims),
        out_shape=jax.ShapeDtypeStruct((toks, LANES), BF),
        in_specs=[vmem] * 5 + [hbm] * 3,
        out_specs=vmem,
        scratch_shapes=[
            pltpu.VMEM((2 * hid_pad, width), BF),
            pltpu.VMEM((hid_pad, width), BF),
            pltpu.VMEM((n_ep, toks), F32),
            pltpu.VMEM((toks, 8), F32),
            pltpu.VMEM((3, n_ep, cap, LANES), BF),
            pltpu.VMEM((n_tp, 1, LANES), F32),
            pltpu.VMEM((n_tp, n_ep * cap, LANES), BF),
            pltpu.VMEM((rows, width), BF),
            pltpu.VMEM((rows, hid_pad), BF),
            pltpu.VMEM((chunks, 2, nz, rows, LANES), BF),
            pltpu.VMEM((chunks, nz, rows, LANES), BF),
            pltpu.VMEM((chunks, 2, hops, rows, LANES), BF),
            pltpu.VMEM((chunks, 2, hops, rows, LANES), BF),
            pltpu.VMEM((3, n_ep * cap, LANES), BF),
            pltpu.VMEM((3, n_ep * cap, LANES), BF),
            pltpu.VMEM((2, toks, LANES), F32),
            pltpu.VMEM((n_tp, 1, toks), F32),
            pltpu.VMEM((1, toks), F32),
            pltpu.VMEM((2, toks, LANES), BF),
            pltpu.VMEM((2, toks, 2 * LANES), F32),
            pltpu.VMEM((2, toks, LANES), BF),
            pltpu.VMEM((2, toks, LANES), BF),
            pltpu.VMEM((rows, LANES), F32),
            dma((3,)),
            dma, dma,
            dma, dma((n_ep,)),
            dma((chunks,)), dma((TURNS, 2, hops, 2)), dma, dma((chunks,)),
            dma, dma((TURNS,)),
            dma((chunks,)), dma((TURNS, 2, hops, 2)),
            dma, dma((n_ep,)),
            dma, dma,
            dma((2,)), dma((2,)),
            dma, dma((chunks,)),
            dma, dma((chunks,)),
            dma((2,)), dma((2,)),
        ],
        compiler_params=pltpu.CompilerParams(
            collective_id=0, has_side_effects=True, vmem_limit_bytes=66_000_000
        ),
        name="experts",
    )


def on_device(dims, tokens, pre_gain, ids, weights, gate_weight, up_weight, down_weight, post_gain):
    call = make(dims, tokens.shape[0], gate_weight.shape[2])
    return call(
        tokens, ids.T, weights.T, pre_gain[None], post_gain[None],
        gate_weight[0].T, up_weight[0].T, down_weight[0],
    )


def build(mesh, dims):
    placed = (
        P("ep", "tp"),
        P("tp"),
        P("ep", None),
        P("ep", None),
        P("ep", None, "tp"),
        P("ep", None, "tp"),
        P("ep", "tp", None),
        P("tp"),
    )
    return jax.shard_map(
        functools.partial(on_device, dims), mesh=mesh, in_specs=placed, out_specs=P("ep", "tp"), check_vma=False
    )


def solution(mesh):
    n_ep, n_tp = mesh.shape["ep"], mesh.shape["tp"]
    return build(mesh, (n_ep // NX, NX, n_tp // 2, 144, 2, 128 * n_tp, 2, 8))
```

```python
import functools

import jax
import jax.numpy as jnp
from jax import lax
from jax.experimental import pallas as pl
from jax.experimental.pallas import tpu as pltpu
from jax.sharding import PartitionSpec as P

BF, F32 = jnp.bfloat16, jnp.float32
MESH = pl.DeviceIdType.MESH
NX = 4
EPS = 1e-06
LANES = 128
TURNS = 4
FOLD_AT = 1
NT = (((1,), (1,)), ((), ()))


def near_first(i, n):
    return i if n < 4 else i + lax.div(i, 2) - 2 * lax.div(i, 3)


def kernel(
    dims,
    tokens, ids, weights, pre_gain, post_gain, gate_hbm, up_hbm, down_hbm,
    out,
    gates, downs, ranks, cols, outgoing, gains, x_all, x_norm, hidden,
    part, peer_part, ring_out, ring_in, results, returned, sums, squares, square_own,
    tok_near, near_sums, near_out, near_in, row_scale,
    w_sem, gain_s, gain_r, disp_s, disp_r, ag_s, ag_r, d2d_s, d2d_r,
    pp_s, pp_r, rs_s, rs_r, ret_s, ret_r, sq_s, sq_r,
    tn_s, tn_r, near_s, near_r, nret_s, nret_r, nx_s, nx_r,
):
    ny, nx, nz, cap, per_chunk, width, plain_in, plain_out = dims
    n_ep, n_tp = ny * nx, nz * 2
    chunks = n_ep // per_chunk
    rows = cap * per_chunk
    near_out_chunks = chunks - plain_out
    half = -(-rows // 32) * 16
    hops = nz // 2
    toks = tokens.shape[0]
    hid = gate_hbm.shape[0]
    hid_pad = downs.shape[0]

    ep, tp = lax.axis_index("ep"), lax.axis_index("tp")
    y, x = lax.div(ep, nx), lax.rem(ep, nx)
    z, core = lax.div(tp, 2), lax.rem(tp, 2)
    peer = z * 2 + 1 - core
    right = lax.rem(z + 1, nz) * 2 + core
    left = lax.rem(z + nz - 1, nz) * 2 + core

    def remote(src, dst, ssem, rsem, ep_to, tp_to):
        return pltpu.make_async_remote_copy(
            src_ref=src, dst_ref=dst, send_sem=ssem, recv_sem=rsem,
            device_id=(ep_to, tp_to), device_id_type=MESH,
        )

    def arrived(ref, sem):
        pltpu.make_async_copy(ref, ref, sem).wait()

    barrier = pltpu.get_barrier_semaphore()

    def greet_ep(i, _):
        pl.semaphore_signal(barrier, inc=1, device_id=(lax.rem(ep + i, n_ep), tp), device_id_type=MESH)
        return 0

    def greet_tp(i, _):
        pl.semaphore_signal(barrier, inc=1, device_id=(ep, lax.rem(tp + i, n_tp)), device_id_type=MESH)
        return 0

    lax.fori_loop(1, n_ep, greet_ep, 0)
    lax.fori_loop(1, n_tp, greet_tp, 0)

    loads = (
        pltpu.make_async_copy(gate_hbm, gates.at[pl.ds(0, hid)], w_sem.at[0]),
        pltpu.make_async_copy(up_hbm, gates.at[pl.ds(hid_pad, hid)], w_sem.at[1]),
        pltpu.make_async_copy(down_hbm, downs.at[pl.ds(0, hid)], w_sem.at[2]),
    )
    for load in loads:
        load.start()
    if hid_pad > hid:
        gates[pl.ds(hid, hid_pad - hid), :] = jnp.zeros((hid_pad - hid, width), BF)
        gates[pl.ds(hid_pad + hid, hid_pad - hid), :] = jnp.zeros((hid_pad - hid, width), BF)
        downs[pl.ds(hid, hid_pad - hid), :] = jnp.zeros((hid_pad - hid, width), BF)
    gains[tp] = pre_gain[...].astype(F32)

    o_i = lax.broadcasted_iota(jnp.int32, (n_ep, toks), 0)
    a_i, b_i = o_i // nx, o_i % nx

    def near_vec(i, n):
        return i if n < 4 else jnp.where(i == 2, 3, jnp.where(i == 3, 2, i))

    e_of = ((y + near_vec(a_i, ny)) % ny) * nx + (x + near_vec(b_i, nx)) % nx
    first = (ids[0:1, :] == e_of).astype(F32)
    second = (ids[1:2, :] == e_of).astype(F32)
    named = first + second
    named_bf = named.astype(BF)
    step = min(256, toks)
    for at in range(0, toks, step):
        before = lax.broadcasted_iota(jnp.int32, (toks, step), 0)
        after = lax.broadcasted_iota(jnp.int32, (toks, step), 1) + at
        upper = jnp.where(before < after, 1.0, 0.0).astype(BF)
        ranks[:, pl.ds(at, step)] = jnp.dot(named_bf, upper, preferred_element_type=F32)
    rank = ranks[...]
    slot = o_i.astype(F32) * float(cap) + rank
    slot0 = jnp.sum(first * slot, axis=0, keepdims=True)
    slot1 = jnp.sum(second * slot, axis=0, keepdims=True)
    ranks[...] = jnp.where(named > 0.0, rank, -1.0)
    r8 = lax.broadcasted_iota(jnp.int32, (8, toks), 0)
    table = jnp.where(r8 == 0, slot0, jnp.where(r8 == 1, slot1, jnp.where(r8 == 2, weights[0:1, :], weights[1:2, :])))
    cols[...] = table.T

    def block_peer(o, sign):
        dy = near_first(lax.div(o, nx), ny)
        dx = near_first(lax.rem(o, nx), nx)
        return lax.rem(y + ny + sign * dy, ny) * nx + lax.rem(x + nx + sign * dx, nx)

    def block_rows(o):
        return pl.ds(pl.multiple_of(o * cap, 16), cap)

    def dispatch_copy(o):
        return remote(
            outgoing.at[0, o], x_all.at[tp, block_rows(o)], disp_s, disp_r.at[o], block_peer(o, 1), tp
        )

    s_i = lax.broadcasted_iota(jnp.int32, (cap, toks), 0).astype(F32)

    def dispatch(o, _):
        pick = jnp.where(s_i == ranks[pl.ds(o, 1), :], 1.0, 0.0).astype(BF)
        picked = jnp.dot(pick, tokens[...], preferred_element_type=F32).astype(BF)

        @pl.when(o == 0)
        def _():
            x_all[tp, pl.ds(0, cap)] = picked

        @pl.when(o > 0)
        def _():
            outgoing[0, o] = picked

        return 0

    lax.fori_loop(0, n_ep, dispatch, 0)

    pl.semaphore_wait(barrier, n_ep - 1 + n_tp - 1)

    def send_gain(i, _):
        remote(gains.at[tp], gains.at[tp], gain_s, gain_r, ep, lax.rem(tp + i, n_tp)).start()
        return 0

    def token_copy(way):
        return remote(
            tokens, tok_near.at[way], tn_s.at[way], tn_r.at[way], ep, right if way == 0 else left
        )

    def send_block(o, _):
        dispatch_copy(o).start()
        return 0

    if plain_in < chunks:
        for way in (0, 1):
            token_copy(way).start()
    lax.fori_loop(1, n_ep, send_block, 0)
    lax.fori_loop(1, n_tp, send_gain, 0)

    def chunk_rows(c, at=0, count=None):
        return pl.ds(pl.multiple_of(c * rows + at, 16), rows if count is None else count)

    def slice_at(h):
        return lax.rem(z + 2 * nz - h, nz) * 2 + core

    def sub_rows(sub):
        return (0, half) if sub == 0 else (half, rows - half)

    def subs_of(h, way):
        return (0, 1) if h < hops else (way,)

    def ag_copy(c, h, way, sub):
        ref = x_all.at[slice_at(h - 1 if way == 0 else 1 - h), chunk_rows(c, *sub_rows(sub))]
        return remote(
            ref, ref, ag_s.at[c], ag_r.at[lax.rem(c, TURNS), way, h - 1, sub], ep, right if way == 0 else left
        )

    def ag_arrived(c, h, way, sub):
        ref = x_all.at[slice_at(h if way == 0 else -h), chunk_rows(c, *sub_rows(sub))]
        remote(ref, ref, ag_s.at[c], ag_r.at[lax.rem(c, TURNS), way, h - 1, sub], ep, right).wait_recv()

    def d2d_copy(c, q):
        ref = x_all.at[slice_at(q), chunk_rows(c)]
        return remote(ref, ref, d2d_s, d2d_r.at[c], ep, peer)

    def near_copy(o, way):
        j = slice_at(1 if way == 0 else -1)
        return remote(
            outgoing.at[1 + way, o], x_all.at[j, block_rows(o)],
            near_s, near_r.at[lax.div(o, per_chunk)], block_peer(o, 1), tp,
        )

    def near_dispatch(c):
        @pl.when(c == plain_in)
        def _():
            for way in (0, 1):
                token_copy(way).wait_recv()

        for b in range(per_chunk):
            o = c * per_chunk + b
            pick = jnp.where(s_i == ranks[pl.ds(o, 1), :], 1.0, 0.0).astype(BF)
            both = jnp.concatenate([tok_near[0], tok_near[1]], axis=1)
            picked = jnp.dot(pick, both, preferred_element_type=F32).astype(BF)
            for way in (0, 1):
                outgoing[1 + way, o] = picked[:, way * LANES:(way + 1) * LANES]
                near_copy(o, way).start()

    def gather_first(c):
        for b in range(per_chunk):
            o = c * per_chunk + b

            @pl.when(o > 0)
            def _():
                dispatch_copy(o).wait_recv()

            if (b + 1) * cap in (half, rows):
                sub = 0 if (b + 1) * cap == half else 1

                @pl.when(c < plain_in)
                def _():
                    for way in (0, 1):
                        for piece in ((0, 1) if per_chunk == 1 else (sub,)):
                            ag_copy(c, 1, way, piece).start()


        d2d_copy(c, 0).start()

    def gather_hop(c, h):
        if h == 1:
            @pl.when(c >= plain_in)
            def _():
                arrived(x_all.at[pl.ds(0, 2), chunk_rows(c)], near_r.at[c])

        for sub in (0, 1):
            for way in (0, 1):
                if sub not in subs_of(h, way):
                    continue
                if h > 1:
                    ag_arrived(c, h, way, sub)
                else:
                    @pl.when(c < plain_in)
                    def _():
                        ag_arrived(c, h, way, sub)

                if h < hops and sub in subs_of(h + 1, way):
                    ag_copy(c, h + 1, way, sub).start()
                if h < hops and sub == 1:
                    d2d_copy(c, h if way == 0 else -h).start()

        if h == hops:
            d2d_copy(c, h).start()

    def fold_gain():
        for load in loads:
            load.wait()
        arrived(gains.at[pl.ds(1, n_tp - 1)], gain_r)
        gain = jnp.concatenate([gains[j] for j in range(n_tp)], axis=1)
        block = 64

        def fold(i, _):
            at = pl.ds(pl.multiple_of(i * block, block), block)
            gates[at, :] = (gates[at, :].astype(F32) * gain).astype(BF)
            return 0

        lax.fori_loop(0, 2 * hid_pad // block, fold, 0)

    def feed_forward(c):
        arrived(x_all.at[pl.ds(0, nz), chunk_rows(c)], d2d_r.at[c])

        def squares_of(i, _):
            at = pl.ds(pl.multiple_of(c * rows + i * 16, 16), 16)
            to = pl.ds(pl.multiple_of(i * 16, 16), 16)
            total = jnp.zeros((16, LANES), F32)
            for j in range(n_tp):
                raw = x_all[j, at]
                x_norm[to, j * LANES:(j + 1) * LANES] = raw
                v = raw.astype(F32)
                total = total + v * v
            mean = jnp.sum(total, axis=1, keepdims=True) / width
            row_scale[to, :] = jnp.broadcast_to(lax.rsqrt(mean + EPS), (16, LANES))
            return 0

        lax.fori_loop(0, rows // 16, squares_of, 0, unroll=3 if rows % 48 == 0 else 1)
    tile = min(256, hid_pad)

    def project(c, at):
        g = lax.dot_general(x_norm[...], gates[at:at + tile, :], NT, preferred_element_type=F32)
        u = lax.dot_general(x_norm[...], gates[hid_pad + at:hid_pad + at + tile, :], NT, preferred_element_type=F32)
        scale = jnp.concatenate([row_scale[...]] * (tile // LANES), axis=1)
        g, u = g * scale, u * scale
        hidden[:, at:at + tile] = (g / (1.0 + jnp.exp(-g)) * u).astype(BF)

    def project_down(c):
        for m in range(nz):
            p = jnp.dot(hidden[...], downs[:, m * 256:(m + 1) * 256], preferred_element_type=F32).astype(BF)
            part[c, 0, m] = p[:, :LANES]
            part[c, 1, m] = p[:, LANES:]
        peer_copy(c).start()

    def peer_copy(c):
        return remote(part.at[c, 1 - core], peer_part.at[c], pp_s, pp_r.at[lax.rem(c, TURNS)], ep, peer)

    def chip_sum(c, zd, at=0, count=None):
        sl = pl.ds(at, rows if count is None else count)
        return part[c, core, zd, sl, :].astype(F32) + peer_part[c, zd, sl, :].astype(F32)

    def rs_subs(s, way):
        return (0, 1) if s > 1 else (way,)

    def rs_copy(c, s, way, sub):
        sl = pl.ds(*sub_rows(sub))
        return remote(
            ring_out.at[c, way, s - 1, sl], ring_in.at[c, way, s - 1, sl],
            rs_s.at[c], rs_r.at[lax.rem(c, TURNS), way, s - 1, sub], ep, right if way == 0 else left,
        )

    def scatter_stage(c, s):
        if s == 1:
            peer_copy(c).wait_recv()
        far = hops + 1 - s
        for sub in (0, 1):
            at, count = sub_rows(sub)
            for way in (0, 1):
                if sub not in rs_subs(s, way):
                    continue
                zd = lax.rem(z + far, nz) if way == 0 else lax.rem(z + nz - far, nz)
                v = chip_sum(c, zd, at, count)
                if s > 1 and sub in rs_subs(s - 1, way):
                    rs_copy(c, s - 1, way, sub).wait_recv()
                    v = v + ring_in[c, way, s - 2, at:at + count, :].astype(F32)
                ring_out[c, way, s - 1, at:at + count, :] = v.astype(BF)
                rs_copy(c, s, way, sub).start()

    def stage_arrived(c, s):
        for sub in (0, 1):
            for way in (0, 1):
                if sub in rs_subs(s, way):
                    rs_copy(c, s, way, sub).wait_recv()

    def return_copy(o):
        return remote(
            results.at[0, block_rows(o)], returned.at[0, block_rows(o)], ret_s, ret_r.at[o], block_peer(o, -1), tp
        )

    def near_return_copy(o, way):
        return remote(
            results.at[1 + way, block_rows(o)], returned.at[1 + way, block_rows(o)],
            nret_s, nret_r.at[lax.div(o, per_chunk)], block_peer(o, -1), tp,
        )

    def last_hop(c):
        @pl.when(c >= near_out_chunks)
        def _():
            scatter_stage(c, hops)

        @pl.when(c < near_out_chunks)
        def _():
            stage_arrived(c, hops - 1)
            for b in range(per_chunk):
                o = c * per_chunk + b
                at = b * cap
                own = chip_sum(c, z, at, cap).astype(BF)
                near = []
                for way in (0, 1):
                    zd = lax.rem(z + 1, nz) if way == 0 else lax.rem(z + nz - 1, nz)
                    v = chip_sum(c, zd, at, cap) + ring_in[c, way, hops - 2, at:at + cap, :].astype(F32)
                    near.append(v.astype(BF))

                @pl.when(o == 0)
                def _():
                    returned[0, pl.ds(0, cap), :] = own
                    for way in (0, 1):
                        returned[1 + way, pl.ds(0, cap), :] = near[way]

                @pl.when(o > 0)
                def _():
                    results[0, block_rows(o), :] = own
                    return_copy(o).start()
                    for way in (0, 1):
                        results[1 + way, block_rows(o), :] = near[way]
                        near_return_copy(o, way).start()

    def finish(c):
        @pl.when(c < near_out_chunks)
        def _():
            combine(c, True)

        @pl.when(c >= near_out_chunks)
        def _():
            stage_arrived(c, hops)
            for b in range(per_chunk):
                o = c * per_chunk + b
                at = b * cap
                v = chip_sum(c, z, at, cap)
                for way in (0, 1):
                    v = v + ring_in[c, way, hops - 1, at:at + cap, :].astype(F32)
                v = v.astype(BF)

                @pl.when(o == 0)
                def _():
                    returned[0, pl.ds(0, cap), :] = v

                @pl.when(o > 0)
                def _():
                    results[0, block_rows(o), :] = v
                    return_copy(o).start()

    def near_sum_copy(way):
        return remote(
            near_out.at[way], near_in.at[way], nx_s.at[way], nx_r.at[way], ep, right if way == 0 else left
        )

    def combine(c, near):
        for b in range(per_chunk):
            o = c * per_chunk + b

            @pl.when(o > 0)
            def _():
                return_copy(o).wait_recv()

        lane = lax.broadcasted_iota(jnp.int32, (toks, rows), 1).astype(F32) + (c * rows).astype(F32)
        values = returned[0, chunk_rows(c), :]
        if near:
            @pl.when(c > 0)
            def _():
                arrived(x_all.at[pl.ds(0, 2), chunk_rows(c)], nret_r.at[c])

            @pl.when(c == 0)
            def _():
                if per_chunk > 1:
                    arrived(x_all.at[pl.ds(0, 2), pl.ds(0, rows - cap)], nret_r.at[c])

            values = jnp.concatenate([values, returned[1, chunk_rows(c), :], returned[2, chunk_rows(c), :]], axis=1)
        for k in (0, 1):
            pick = jnp.where(lane == cols[:, k:k + 1], 1.0, 0.0).astype(BF)
            got = jnp.dot(pick, values, preferred_element_type=F32)

            @pl.when(c == 0)
            def _():
                sums[k] = got[:, :LANES]
                if near:
                    near_sums[k] = got[:, LANES:]

            @pl.when(c > 0)
            def _():
                sums[k] = sums[k] + got[:, :LANES]
                if near:
                    near_sums[k] = near_sums[k] + got[:, LANES:]

        if near:
            @pl.when(c == near_out_chunks - 1)
            def _():
                total = cols[:, 2:3] * near_sums[0] + cols[:, 3:4] * near_sums[1]
                for way in (0, 1):
                    near_out[way] = total[:, way * LANES:(way + 1) * LANES].astype(BF)
                    near_sum_copy(way).start()

    def last_combine(c):
        @pl.when(c >= near_out_chunks)
        def _():
            combine(c, False)

    stages = [(gather_first, 0)]
    hop = [(functools.partial(gather_hop, h=h), h) for h in range(1, hops + 1)]
    forward = [feed_forward] + [functools.partial(project, at=at) for at in range(0, hid_pad, tile)] + [project_down]
    forward = [(part_of, hops + 1) for part_of in forward]
    while hop or forward:
        stages += hop[:1] + forward[:1]
        hop, forward = hop[1:], forward[1:]
    if plain_in < chunks:
        stages += [(near_dispatch, -1)]
    stages += [(functools.partial(scatter_stage, s=s), hops + 1 + s) for s in range(1, hops)]
    stages += [(last_hop, 2 * hops + 1), (finish, 2 * hops + 2), (last_combine, 2 * hops + 3)]

    def slot_step(t, _):
        @pl.when(t == FOLD_AT)
        def _():
            fold_gain()

        for stage, first_slot in stages:
            c = t - first_slot
            low = plain_in if stage is near_dispatch else 0

            @pl.when((c >= low) & (c < chunks))
            def _():
                stage(c)

        return 0

    lax.fori_loop(0, chunks + 2 * hops + 3, slot_step, 0)

    both = cols[:, 2:3] * sums[0] + cols[:, 3:4] * sums[1]
    if near_out_chunks:
        for way in (0, 1):
            near_sum_copy(way).wait_recv()
            both = both + near_in[way].astype(F32)
    sums[0] = both
    square_own[...] = jnp.sum((both * both).T, axis=0, keepdims=True)

    def square_copy(i):
        return remote(square_own, squares.at[i], sq_s, sq_r, ep, lax.rem(tp + i, n_tp))

    def send_square(i, _):
        square_copy(i).start()
        return 0

    lax.fori_loop(1, n_tp, send_square, 0)

    arrived(gains.at[pl.ds(1, n_tp - 1)], gain_s)
    arrived(outgoing.at[0, pl.ds(1, n_ep - 1)], disp_s)
    arrived(results.at[0, pl.ds(cap, (n_ep - 1) * cap)], ret_s)
    arrived(x_all.at[pl.ds(0, nz)], d2d_s)
    arrived(x_all.at[pl.ds(0, nz)], pp_s)
    for c in range(chunks):
        arrived(part.at[c, 0, pl.ds(0, nz - 1 if c < plain_in else nz - 3)], ag_s.at[c])
        arrived(part.at[c, 0, pl.ds(0, nz - 3 if c < near_out_chunks else nz - 1)], rs_s.at[c])
    first_near = plain_in * per_chunk
    if first_near < n_ep:
        arrived(outgoing.at[pl.ds(1, 2), pl.ds(first_near, n_ep - first_near)], near_s)
    last_near = near_out_chunks * per_chunk
    if last_near > 1:
        arrived(results.at[pl.ds(1, 2), pl.ds(cap, (last_near - 1) * cap)], nret_s)
    for way in (0, 1):
        if plain_in < chunks:
            token_copy(way).wait_send()
        if near_out_chunks:
            near_sum_copy(way).wait_send()

    total = square_own[...]
    arrived(squares.at[pl.ds(1, n_tp - 1)], sq_r)
    for i in range(1, n_tp):
        total = total + squares[i]
    scale = lax.rsqrt(total / width + EPS)
    scale = jnp.broadcast_to(scale, (8, toks)).T
    out[...] = (sums[0] * scale[:, 0:1] * post_gain[...].astype(F32)).astype(BF)

    arrived(squares.at[pl.ds(1, n_tp - 1)], sq_s)


def make(dims, toks, hid):
    ny, nx, nz, cap, per_chunk, width, _, _ = dims
    n_ep, n_tp = ny * nx, nz * 2
    chunks, rows, hops = n_ep // per_chunk, cap * per_chunk, nz // 2
    hid_pad = -(-hid // 256) * 256 if hid > 128 else 128
    vmem = pl.BlockSpec(memory_space=pltpu.VMEM)
    hbm = pl.BlockSpec(memory_space=pl.ANY)
    dma = pltpu.SemaphoreType.DMA
    return pl.pallas_call(
        functools.partial(kernel, dims),
        out_shape=jax.ShapeDtypeStruct((toks, LANES), BF),
        in_specs=[vmem] * 5 + [hbm] * 3,
        out_specs=vmem,
        scratch_shapes=[
            pltpu.VMEM((2 * hid_pad, width), BF),
            pltpu.VMEM((hid_pad, width), BF),
            pltpu.VMEM((n_ep, toks), F32),
            pltpu.VMEM((toks, 8), F32),
            pltpu.VMEM((3, n_ep, cap, LANES), BF),
            pltpu.VMEM((n_tp, 1, LANES), F32),
            pltpu.VMEM((n_tp, n_ep * cap, LANES), BF),
            pltpu.VMEM((rows, width), BF),
            pltpu.VMEM((rows, hid_pad), BF),
            pltpu.VMEM((chunks, 2, nz, rows, LANES), BF),
            pltpu.VMEM((chunks, nz, rows, LANES), BF),
            pltpu.VMEM((chunks, 2, hops, rows, LANES), BF),
            pltpu.VMEM((chunks, 2, hops, rows, LANES), BF),
            pltpu.VMEM((3, n_ep * cap, LANES), BF),
            pltpu.VMEM((3, n_ep * cap, LANES), BF),
            pltpu.VMEM((2, toks, LANES), F32),
            pltpu.VMEM((n_tp, 1, toks), F32),
            pltpu.VMEM((1, toks), F32),
            pltpu.VMEM((2, toks, LANES), BF),
            pltpu.VMEM((2, toks, 2 * LANES), F32),
            pltpu.VMEM((2, toks, LANES), BF),
            pltpu.VMEM((2, toks, LANES), BF),
            pltpu.VMEM((rows, LANES), F32),
            dma((3,)),
            dma, dma,
            dma, dma((n_ep,)),
            dma((chunks,)), dma((TURNS, 2, hops, 2)), dma, dma((chunks,)),
            dma, dma((TURNS,)),
            dma((chunks,)), dma((TURNS, 2, hops, 2)),
            dma, dma((n_ep,)),
            dma, dma,
            dma((2,)), dma((2,)),
            dma, dma((chunks,)),
            dma, dma((chunks,)),
            dma((2,)), dma((2,)),
        ],
        compiler_params=pltpu.CompilerParams(
            collective_id=0, has_side_effects=True, vmem_limit_bytes=66_000_000
        ),
        name="experts",
    )


def on_device(dims, tokens, pre_gain, ids, weights, gate_weight, up_weight, down_weight, post_gain):
    call = make(dims, tokens.shape[0], gate_weight.shape[2])
    return call(
        tokens, ids.T, weights.T, pre_gain[None], post_gain[None],
        gate_weight[0].T, up_weight[0].T, down_weight[0],
    )


def build(mesh, dims):
    placed = (
        P("ep", "tp"),
        P("tp"),
        P("ep", None),
        P("ep", None),
        P("ep", None, "tp"),
        P("ep", None, "tp"),
        P("ep", "tp", None),
        P("tp"),
    )
    return jax.shard_map(
        functools.partial(on_device, dims), mesh=mesh, in_specs=placed, out_specs=P("ep", "tp"), check_vma=False
    )


def solution(mesh):
    n_ep, n_tp = mesh.shape["ep"], mesh.shape["tp"]
    return build(mesh, (n_ep // NX, NX, n_tp // 2, 144, 2, 128 * n_tp, 2, 8))
```
